1024 devices in a mesh: sp: 16 (over z), tp: 64 (over y, x, core).
Axes of the slice: x: 4, y: 8, z: 16, core: 2. Of those that a mesh axis runs over, the one named last changes fastest.
Arguments:
- latent: bfloat16 [4096, 4096], P(('sp', 'tp')), may hold values from -16 to 16
- context: bfloat16 [256, 4096], P('sp'), may hold values from -16 to 16
- cond: bfloat16 [4096], P('sp'), may hold values from -6 to 6
- cond_ctx: bfloat16 [4096], P('sp'), may hold values from -6 to 6
- mod_shift_w: bfloat16 [4096, 4096], P('sp', 'tp'), may hold values from -0.15625 to 0.15625
- mod_scale_w: bfloat16 [4096, 4096], P('sp', 'tp'), may hold values from -0.15625 to 0.15625
- mod_gate_w: bfloat16 [4096, 4096], P('sp', 'tp'), may hold values from -0.15625 to 0.15625
- norm_gain: bfloat16 [4096], replicated, may hold values from 0.099609375 to 1.8984375
- proj_z: bfloat16 [4096, 4096], P(None, 'tp'), may hold values from -0.09375 to 0.09375
- proj_x: bfloat16 [4096, 4096], P(None, 'tp'), may hold values from -0.09375 to 0.09375
- proj_b: bfloat16 [4096, 8192], P(None, 'tp'), may hold values from -0.09375 to 0.09375
- proj_c: bfloat16 [4096, 8192], P(None, 'tp'), may hold values from -0.09375 to 0.09375
- proj_dt: bfloat16 [4096, 128], replicated, may hold values from -0.09375 to 0.09375
- conv_x: bfloat16 [3, 4096], P(None, 'tp'), may hold values from -3.5 to 3.5
- conv_b: bfloat16 [3, 8192], P(None, 'tp'), may hold values from -3.5 to 3.5
- conv_c: bfloat16 [3, 8192], P(None, 'tp'), may hold values from -3.5 to 3.5
- dt_bias: float32 [128], P('tp'), may hold values from -1 to 1
- decay_log: float32 [128], P('tp'), may hold values from -11.6 to -2.9
- head_gain: bfloat16 [4096], P('tp'), may hold values from 0.099609375 to 1.8984375
- proj_out: bfloat16 [4096, 4096], P(None, 'tp'), may hold values from -0.09375 to 0.09375
Outputs:
- mixed: bfloat16 [4096, 4096], P(('sp', 'tp'))
The draws below stay inside these ranges and needn't reach their ends.
All inputs are finite; a program needn't handle non-finite values.
Results may differ from the reference program's by a relative error of at most 0.0065.
Values may be sent and summed in bfloat16 or wider, within the bound.
A program may use at most 64 MiB of HBM per device.

```python
import jax
import jax.numpy as jnp
from jax import lax

D = 4096
HEADS = 64
HEAD_DIM = 64
STATE = 128
BLOCK = 128
CTX = 256
SEQ = 4096


def draw_latent(key, part):
    key_noise = jax.random.fold_in(key, 11)
    key_dir = jax.random.fold_in(key, 12)
    key_level = jax.random.fold_in(key, 13)
    direction = jax.random.normal(key_dir, (D,), jnp.float32)
    levels = jax.random.uniform(key_level, (SEQ // BLOCK,), jnp.float32, -1.5, 1.5)
    offsets = jnp.repeat(levels, BLOCK, total_repeat_length=SEQ)[:, None] * direction[None, :]
    noise = jax.random.normal(key_noise, (SEQ, D), jnp.float32)
    return jnp.clip(noise + offsets, -16.0, 16.0).astype(jnp.bfloat16)


def draw_context(key, part):
    key_noise = jax.random.fold_in(key, 31)
    key_seg = jax.random.fold_in(key, 32)
    segment = CTX // 16
    directions = jax.random.normal(key_seg, (16, D), jnp.float32) * 4.0
    offsets = jnp.repeat(directions, segment, axis=0, total_repeat_length=CTX)
    noise = jax.random.normal(key_noise, (CTX, D), jnp.float32) * 0.7
    return jnp.clip(noise + offsets, -16.0, 16.0).astype(jnp.bfloat16)


def draw_decay_log(key, part):
    key_pick = jax.random.fold_in(key, 21)
    key_slow = jax.random.fold_in(key, 22)
    key_fast = jax.random.fold_in(key, 23)
    slow = jax.random.uniform(key_slow, (2 * HEADS,), jnp.float32, -11.5, -9.45)
    fast = jax.random.uniform(key_fast, (2 * HEADS,), jnp.float32, -4.2, -3.0)
    share = 0.5
    pick = jax.random.uniform(key_pick, (2 * HEADS,), jnp.float32) < share
    return jnp.where(pick, fast, slow)


def shard_levels(key, dims, shards, least, largest):
    level, own = 1.0, jax.random.fold_in(key, 6)
    for axis_at, blocks in shards:
        draws = jnp.exp(jax.random.uniform(jax.random.fold_in(own, axis_at), (blocks,), jnp.float32, least / len(shards), largest / len(shards)))
        level = level * jnp.repeat(draws, dims[axis_at] // blocks).reshape([-1 if axis == axis_at else 1 for axis in range(len(dims))])
    return level


def scatter_about(rng, shape, deviation, most, split=(), dtype=jnp.bfloat16):
    loudness = shard_levels(rng, shape, split, -0.22, 0.18) if split else 1.0
    array = jax.random.normal(rng, shape, jnp.float32) * deviation * loudness
    return jnp.minimum(jnp.maximum(array, -most), most).astype(dtype)


def setup_inputs(seed: int = 0) -> dict:
    keys = jax.random.split(jax.random.key(seed), 21)
    latent = draw_latent(jax.random.fold_in(keys[20], 71), 0)
    context = draw_context(jax.random.fold_in(keys[20], 71), 0)
    cond = scatter_about(keys[2], (D,), 1.0, 6.0, ((0, 16),))
    cond_ctx = scatter_about(keys[3], (D,), 1.0, 6.0, ((0, 16),))
    mod_shift_w = scatter_about(keys[4], (D, D), (D // 3) ** -0.5, 0.15625, ((0, 16), (1, 64)))
    mod_scale_w = scatter_about(keys[5], (D, D), (D // 3) ** -0.5, 0.15625, ((0, 16), (1, 64)))
    mod_gate_w = scatter_about(keys[6], (D, D), (D // 3) ** -0.5, 0.15625, ((0, 16), (1, 64)))
    norm_gain = jnp.clip(1.0 + 0.18 * jax.random.normal(keys[7], (D,), jnp.float32), 0.099609375, 1.8984375).astype(jnp.bfloat16)
    proj_z = scatter_about(keys[8], (D, D), D ** -0.5, 0.09375, ((1, 64),))
    proj_x = scatter_about(keys[9], (D, D), D ** -0.5, 0.09375, ((1, 64),))
    proj_b = scatter_about(keys[10], (D, HEADS * STATE), D ** -0.5, 0.09375, ((1, 64),))
    proj_c = scatter_about(keys[11], (D, HEADS * STATE), D ** -0.5, 0.09375, ((1, 64),))
    proj_dt = scatter_about(keys[12], (D, 2 * HEADS), D ** -0.5, 0.09375)
    conv_x = scatter_about(keys[13], (3, D), 3 ** -0.5, 3.5, ((1, 64),))
    conv_b = scatter_about(keys[14], (3, HEADS * STATE), 3 ** -0.5, 3.5, ((1, 64),))
    conv_c = scatter_about(keys[15], (3, HEADS * STATE), 3 ** -0.5, 3.5, ((1, 64),))
    dt_bias = jnp.clip(jax.random.uniform(keys[16], (2 * HEADS,), jnp.float32, -1.0, 1.0) * shard_levels(keys[16], (2 * HEADS,), ((0, 64),), -0.4, 0.0), -1.0, 1.0)
    decay_log = draw_decay_log(jax.random.fold_in(keys[20], 71), 0)
    head_gain = jnp.clip(1.0 + 0.18 * jax.random.normal(keys[18], (D,), jnp.float32), 0.099609375, 1.8984375).astype(jnp.bfloat16)
    proj_out = scatter_about(keys[19], (D, D), D ** -0.5, 0.09375, ((1, 64),))
    return dict(latent=latent, context=context, cond=cond, cond_ctx=cond_ctx, mod_shift_w=mod_shift_w, mod_scale_w=mod_scale_w, mod_gate_w=mod_gate_w, norm_gain=norm_gain, proj_z=proj_z, proj_x=proj_x, proj_b=proj_b, proj_c=proj_c, proj_dt=proj_dt, conv_x=conv_x, conv_b=conv_b, conv_c=conv_c, dt_bias=dt_bias, decay_log=decay_log, head_gain=head_gain, proj_out=proj_out)


EPS = 1e-06

def modulated_norm(rows, gain, shift, scale):
    wide = rows.astype(jnp.float32)
    normed = wide * lax.rsqrt(lax.optimization_barrier(jnp.mean(wide * wide, axis=-1, keepdims=True)) + EPS) * gain.astype(jnp.float32)
    return (normed * (1.0 + scale) + shift).astype(jnp.bfloat16)

def project(rows, weights):
    outputs = [jnp.dot(rows, w, preferred_element_type=jnp.float32).astype(jnp.bfloat16) for w in weights]
    return lax.optimization_barrier(outputs)

def centred_conv(padded, taps):
    wide = padded.astype(jnp.float32)
    weights = taps.astype(jnp.float32)
    length = padded.shape[0] - 2
    return jax.nn.silu(weights[0] * wide[:length] + weights[1] * wide[1:length + 1] + weights[2] * wide[2:])

def zero_pad(values):
    return jnp.pad(values, ((1, 1), (0, 0)))

def block_states(values, writes, step_size, decay_rate, block):
    length, heads, width = values.shape
    state = writes.shape[2]
    count = length // block
    log_decay = jnp.cumsum(-(step_size * decay_rate).reshape(count, block, heads), axis=1)
    scaled_values = (values * step_size[:, :, None]).reshape(count, block, heads, width)
    write_blocks = writes.reshape(count, block, heads, state)
    tail = jnp.exp(log_decay[:, -1:] - log_decay)
    block_sums = jnp.einsum('kshn,ksh,kshp->khpn', write_blocks, tail, scaled_values, precision=lax.Precision.HIGHEST)
    block_decay = jnp.exp(log_decay[:, -1])

    def advance(carry, inputs):
        block_sum, decay = inputs
        return (carry * decay[:, None, None] + block_sum, carry)
    final, entering = lax.scan(advance, jnp.zeros((heads, width, state), jnp.float32), (block_sums, block_decay))
    overall = jnp.exp(lax.optimization_barrier(jnp.sum(log_decay[:, -1], axis=0)))
    return (log_decay, scaled_values, entering, final, overall)

def block_outputs(reads, writes, log_decay, scaled_values, entering, start_state):
    count, block, heads = log_decay.shape
    state = reads.shape[2]
    read_blocks = reads.reshape(count, block, heads, state)
    write_blocks = writes.reshape(count, block, heads, state)
    starts = jnp.cumsum(log_decay[:, -1], axis=0) - log_decay[:, -1]
    entering_all = entering + jnp.exp(starts)[:, :, None, None] * start_state[None]
    forward_mask = jnp.tril(jnp.ones((block, block), bool))[None, :, :, None]
    spans = log_decay[:, :, None, :] - log_decay[:, None, :, :]
    weights = jnp.where(forward_mask, jnp.exp(jnp.where(forward_mask, spans, 0.0)), 0.0)
    intersection = jnp.einsum('kqhn,kshn->kqsh', read_blocks, write_blocks, precision=lax.Precision.HIGHEST)
    within = jnp.einsum('kqsh,kshp->kqhp', intersection * weights, scaled_values, precision=lax.Precision.HIGHEST)
    carried = jnp.einsum('kqhn,khpn->kqhp', read_blocks, entering_all, precision=lax.Precision.HIGHEST) * jnp.exp(log_decay)[..., None]
    return (within + carried).reshape(count * block, heads, -1)

def reference(latent, context, cond, cond_ctx, mod_shift_w, mod_scale_w, mod_gate_w, norm_gain, proj_z, proj_x, proj_b, proj_c, proj_dt, conv_x, conv_b, conv_c, dt_bias, decay_log, head_gain, proj_out):
    act = jax.nn.silu(cond.astype(jnp.float32)).astype(jnp.bfloat16)
    act_ctx = jax.nn.silu(cond_ctx.astype(jnp.float32)).astype(jnp.bfloat16)
    shift = jnp.dot(act, mod_shift_w, preferred_element_type=jnp.float32)
    scale = jnp.dot(act, mod_scale_w, preferred_element_type=jnp.float32)
    gate = jnp.dot(act, mod_gate_w, preferred_element_type=jnp.float32)
    ctx_shift = jnp.dot(act_ctx, mod_shift_w, preferred_element_type=jnp.float32)
    ctx_scale = jnp.dot(act_ctx, mod_scale_w, preferred_element_type=jnp.float32)
    normed_rows = modulated_norm(latent, norm_gain, shift, scale)
    normed_ctx = modulated_norm(context, norm_gain, ctx_shift, ctx_scale)
    x_in, b_in, c_in, z_in, dt_raw = project(normed_rows, (proj_x, proj_b, proj_c, proj_z, proj_dt))
    x_ctx, b_ctx, dt_ctx = project(normed_ctx, (proj_x, proj_b, proj_dt))
    values = centred_conv(zero_pad(x_in), conv_x).reshape(SEQ, HEADS, HEAD_DIM)
    writes = centred_conv(zero_pad(b_in), conv_b).reshape(SEQ, HEADS, STATE)
    reads = centred_conv(zero_pad(c_in), conv_c).reshape(SEQ, HEADS, STATE)
    values_ctx = centred_conv(zero_pad(x_ctx), conv_x).reshape(CTX, HEADS, HEAD_DIM)
    writes_ctx = centred_conv(zero_pad(b_ctx), conv_b).reshape(CTX, HEADS, STATE)
    step_size = jax.nn.softplus(dt_raw.astype(jnp.float32) + dt_bias).reshape(SEQ, HEADS, 2)
    step_ctx = jax.nn.softplus(dt_ctx.astype(jnp.float32) + dt_bias).reshape(CTX, HEADS, 2)
    decay_rate = jnp.exp(decay_log).reshape(HEADS, 2)
    ctx_f = block_states(values_ctx, writes_ctx, step_ctx[:, :, 0], decay_rate[:, 0], BLOCK)[3]
    ctx_b = block_states(jnp.flip(values_ctx, 0), jnp.flip(writes_ctx, 0), jnp.flip(step_ctx[:, :, 1], 0), decay_rate[:, 1], BLOCK)[3]
    log_f, scaled_f, enter_f, _, _ = block_states(values, writes, step_size[:, :, 0], decay_rate[:, 0], BLOCK)
    out_f = block_outputs(reads, writes, log_f, scaled_f, enter_f, ctx_f)
    log_b, scaled_b, enter_b, _, _ = block_states(jnp.flip(values, 0), jnp.flip(writes, 0), jnp.flip(step_size[:, :, 1], 0), decay_rate[:, 1], BLOCK)
    out_b = block_outputs(jnp.flip(reads, 0), jnp.flip(writes, 0), log_b, scaled_b, enter_b, ctx_b)
    summed = out_f + jnp.flip(out_b, 0)
    gated = summed * jax.nn.silu(z_in.astype(jnp.float32)).reshape(SEQ, HEADS, HEAD_DIM)
    gated = gated * lax.rsqrt(lax.optimization_barrier(jnp.mean(gated * gated, axis=-1, keepdims=True)) + EPS)
    gated = gated * head_gain.astype(jnp.float32).reshape(HEADS, HEAD_DIM)
    mixed_heads = gated.reshape(SEQ, D).astype(jnp.bfloat16)
    update = jnp.dot(mixed_heads, proj_out, preferred_element_type=jnp.float32).astype(jnp.bfloat16)
    update = lax.optimization_barrier(update).astype(jnp.float32)
    return (latent.astype(jnp.float32) + gate * update).astype(jnp.bfloat16)
```

```python
import functools

import jax
import jax.numpy as jnp
from jax import lax
from jax.experimental import pallas as pl
from jax.experimental.pallas import tpu as pltpu
from jax.sharding import Mesh
from jax.sharding import PartitionSpec as P

TP = ("tp_0", "tp_1", "tp_2")
SP_TP = ("sp", "tp_0", "tp_1", "tp_2")
EPS = 1e-06
MESH_ID = pl.DeviceIdType.MESH
F32 = jnp.float32
BF16 = jnp.bfloat16
HI = lax.Precision.HIGHEST


def iota(shape, dim):
    return lax.broadcasted_iota(jnp.int32, shape, dim)


def silu(v):
    return v * (1.0 / (1.0 + jnp.exp(-v)))


def softplus(v):
    return jnp.maximum(v, 0.0) + jnp.log1p(jnp.exp(-jnp.abs(v)))


def bdot(a, b, dims=(((1,), (0,)), ((), ()))):
    return lax.dot_general(a.astype(BF16), b.astype(BF16), dims, preferred_element_type=F32)


def hdot(a, b):
    return jnp.dot(a, b, precision=HI, preferred_element_type=F32)


def kernel(
    sizes,
    lat_ref, ctx_ref, cond_ref, condc_ref, wsh_ref, wsc_ref, wga_ref, gain_ref,
    pz_ref, px_ref, pb_ref, pc_ref, pdt_ref, cx_ref, cb_ref, cc_ref, dtb_ref, dlog_ref, hg_ref, po_ref,
    out_ref,
    wcat, wx, wz, wo_own, wo_part, wo, latbuf, pbuf, psend, mpair, mpair_r, mbuf, sbuf, acc, accs,
    cbuf, ebuf, esend, lbuf, snd, rst, osend, orecv, obuf, ubuf, rbuf, cst,
    wsem, wosem, worsem, pss, prs, mps, mpr, m1s, m1r, m2s, m2r, lgs, lgr, ld_s, ldr,
    css, csr, es, er, ls_, lr_, sts, str_, ops, opr, ogs, ogr, us, ur,
):
    Z, Y, X = sizes
    NC = Y * X
    HC = NC // 2
    D = lat_ref.shape[1]
    HD = D // 2
    T = NC * 8
    TH = T // 2
    CZ = ctx_ref.shape[0]
    CT = CZ * Z
    z = lax.axis_index("sp")
    y = lax.axis_index("tp_0")
    x = lax.axis_index("tp_1")
    c = lax.axis_index("tp_2")
    chip = y * X + x
    head = chip * 2 + c
    first_core = c == 0

    def remote(src, dst, ssem, rsem, dev):
        return pltpu.make_async_remote_copy(
            src_ref=src, dst_ref=dst, send_sem=ssem, recv_sem=rsem, device_id=dev, device_id_type=MESH_ID
        )

    def drain(ref, sem):
        pltpu.make_async_copy(ref, ref, sem).wait()

    partner = {"tp_2": 1 - c}

    loads = [
        pltpu.make_async_copy(px_ref, wx, wsem.at[0]),
        pltpu.make_async_copy(pz_ref, wz, wsem.at[1]),
        pltpu.make_async_copy(pb_ref, wcat.at[:, 128:256], wsem.at[2]),
        pltpu.make_async_copy(pc_ref, wcat.at[:, 256:384], wsem.at[3]),
        pltpu.make_async_copy(pdt_ref, wcat.at[:, 384:512], wsem.at[4]),
        pltpu.make_async_copy(po_ref, wo_own, wsem.at[5]),
    ]
    for load in loads:
        load.start()

    bar = pltpu.get_barrier_semaphore()

    def greet_z(i, carry):
        pl.semaphore_signal(bar, inc=1, device_id={"sp": lax.rem(z + i, Z)}, device_id_type=MESH_ID)
        return carry

    def greet_plane(i, carry):
        j = lax.rem(chip * 2 + c + i, NC * 2)
        k = j // 2
        pl.semaphore_signal(
            bar, inc=1, device_id={"tp_0": k // X, "tp_1": lax.rem(k, X), "tp_2": lax.rem(j, 2)},
            device_id_type=MESH_ID,
        )
        return carry

    lax.fori_loop(1, Z, greet_z, 0)
    lax.fori_loop(1, NC * 2, greet_plane, 0)

    row8 = iota((8, cond_ref.shape[1]), 0)
    both = jnp.where(row8 == 0, cond_ref[...].astype(F32), jnp.where(row8 == 1, condc_ref[...].astype(F32), 0.0))
    act = silu(both).astype(BF16)

    def wide(part):
        zero = jnp.zeros_like(part)
        return jnp.where(first_core, jnp.concatenate([part, zero], 1), jnp.concatenate([zero, part], 1))

    psh = wide(jnp.dot(act, wsh_ref[...], preferred_element_type=F32))
    psc = wide(jnp.dot(act, wsc_ref[...], preferred_element_type=F32))
    pga = wide(jnp.dot(act, wga_ref[...], preferred_element_type=F32))
    mpair[...] = jnp.concatenate([psh[0:1], psc[0:1], psh[1:2], psc[1:2], pga[0:1]], 0)

    def sq_ctx(k, tot):
        v = ctx_ref[:, pl.ds(pl.multiple_of(k * 128, 128), 128)].astype(F32)
        return tot + v * v

    tot = lax.fori_loop(0, NC, sq_ctx, jnp.zeros((CZ, 128), F32))
    r_ctx = lax.rsqrt(jnp.sum(tot, axis=1, keepdims=True) / D + EPS)

    psend[...] = lat_ref[:, pl.ds(pl.multiple_of((1 - c) * HD, 128), HD)]

    for load in loads[:2]:
        load.wait()
    RB = min(512, D)

    def join_w(i, carry):
        rows = pl.ds(pl.multiple_of(i * RB, RB), RB)
        wcat[rows, 0:128] = jnp.concatenate([wx[rows, :], wz[rows, :]], 1)
        return carry

    lax.fori_loop(0, D // RB, join_w, 0)
    for load in loads[2:]:
        load.wait()

    pl.semaphore_wait(bar, Z - 1 + NC * 2 - 1)

    lp = remote(psend, pbuf, pss, prs, partner)
    lp.start()
    mp = remote(mpair, mpair_r, mps, mpr, partner)
    mp.start()
    wocopy = remote(wo_own, wo_part, wosem, worsem, partner)

    def gather_send(buf, ssem, rsem, slot, dev):
        remote(buf.at[slot], buf.at[slot], ssem, rsem.at[slot], dev).start()

    def gather_wait(buf, ssem, rsem, slot):
        remote(buf.at[slot], buf.at[slot], ssem, rsem.at[slot], partner).wait_recv()

    def along_x(buf, ssem, rsem, slot):
        for d in (1, 3, 2) if X == 4 else range(1, X):
            gather_send(buf, ssem, rsem, slot, {"tp_1": lax.rem(x + d, X)})

    def y_step(i):
        k = i // 2 + 1
        odd = lax.rem(i, 2)
        return lax.rem(y + k * (1 - odd) + (Y - k) * odd, Y)

    def gather_open(buf, ssem, rsem):
        along_x(buf, ssem, rsem, chip)

        def go(i, carry):
            gather_send(buf, ssem, rsem, chip, {"tp_0": y_step(i)})
            return carry

        lax.fori_loop(0, Y - 1, go, 0)

    def gather_relay(buf, ssem, rsem, extra):
        def go(i, carry):
            slot = y_step(i) * X + x
            gather_wait(buf, ssem, rsem, slot)
            along_x(buf, ssem, rsem, slot)
            extra(slot)
            return carry

        lax.fori_loop(0, Y - 1, go, 0)

    def gather_close(buf, ssem, rsem, extra):
        def go(i, carry):
            yy = lax.rem(y + i // (X - 1), Y)
            xx = lax.rem(x + 1 + lax.rem(i, X - 1), X)
            slot = yy * X + xx
            gather_wait(buf, ssem, rsem, slot)
            extra(slot)
            return carry

        lax.fori_loop(0, Y * (X - 1), go, 0)

    def gather_drain(buf, ssem):
        n = Y - 1 + (X - 1) * Y
        drain(buf.at[pl.ds(0, n)], ssem)

    mine = latbuf.at[c]
    other = latbuf.at[1 - c]

    def to_partner(slot):
        remote(mine.at[slot], mine.at[slot], ld_s, ldr.at[slot], partner).start()

    lp.wait_recv()
    got = pbuf[...].astype(F32)
    own = lat_ref[:, pl.ds(pl.multiple_of(c * HD, 128), HD)].astype(F32)
    latbuf[c, chip] = jnp.concatenate(
        [jnp.where(first_core, own, got), jnp.where(first_core, got, own)], 0
    ).astype(BF16)
    gather_open(mine, lgs, lgr)
    to_partner(chip)

    mp.wait_recv()
    mbuf[z] = mpair[...] + mpair_r[...]

    def m1_send(i, carry):
        remote(mbuf.at[z], mbuf.at[z], m1s, m1r.at[z], {"sp": lax.rem(z + i, Z)}).start()
        return carry

    lax.fori_loop(1, Z, m1_send, 0)

    gather_relay(mine, lgs, lgr, to_partner)

    def m1_wait(i, s):
        k = lax.rem(z + i, Z)
        remote(mbuf.at[k], mbuf.at[k], m1s, m1r.at[k], partner).wait_recv()
        return s + mbuf[k]

    msum = lax.fori_loop(1, Z, m1_wait, mbuf[z])
    gate = msum[4:5]
    sbuf[chip] = msum[0:4]

    def m2_send(i, carry):
        k = lax.rem(chip + i, NC)
        remote(
            sbuf.at[chip], sbuf.at[chip], m2s, m2r.at[chip], {"tp_0": k // X, "tp_1": lax.rem(k, X)}
        ).start()
        return carry

    lax.fori_loop(1, NC, m2_send, 0)

    gather_close(mine, lgs, lgr, to_partner)
    wocopy.start()

    def d2d_wait(k, carry):
        remote(other.at[k], other.at[k], ld_s, ldr.at[k], partner).wait_recv()
        return carry

    lax.fori_loop(0, NC, d2d_wait, 0)

    def sq_lat(k, t):
        off = pl.ds(pl.multiple_of(k * 128, 128), 128)
        for h in range(2):
            v = latbuf[h, :, :, off].astype(F32).reshape(T, 128)
            t = t + v * v
        return t

    tot = lax.fori_loop(0, HC, sq_lat, jnp.zeros((T, 128), F32))
    r_lat = lax.rsqrt(jnp.sum(tot, axis=1, keepdims=True) / D + EPS)

    def m2_wait(i, carry):
        k = lax.rem(chip + i, NC)
        remote(sbuf.at[k], sbuf.at[k], m2s, m2r.at[k], partner).wait_recv()
        return carry

    lax.fori_loop(1, NC, m2_wait, 0)

    CH = min(4, HC)
    KB = CH * 128

    def scales(i, row):
        return jnp.concatenate([sbuf[i * CH + j][row : row + 1] for j in range(CH)], 1)

    def chunk(i):
        return i // (HC // CH), pl.multiple_of(lax.rem(i, HC // CH) * KB, 128), pl.multiple_of(i * KB, 128)

    r_first, r_last = r_lat[0:8], r_lat[T - 8 : T]

    def small(i, carry):
        h, off, at = chunk(i)
        gains = gain_ref[:, pl.ds(at, KB)].astype(F32)
        gs = gains * (1.0 + scales(i, 1))
        sh = scales(i, 0)
        gsc = gains * (1.0 + scales(i, 3))
        shc = scales(i, 2)
        vc = ctx_ref[:, pl.ds(at, KB)].astype(F32) * r_ctx * gsc + shc
        v0 = latbuf[h, 0, :, pl.ds(off, KB)].astype(F32) * r_first * gs + sh
        v1 = latbuf[h, NC - 1, :, pl.ds(off, KB)].astype(F32) * r_last * gs + sh
        rows = jnp.concatenate([vc, v0, v1], 0).astype(BF16)
        return carry + jnp.dot(rows, wcat[pl.ds(at, KB), :], preferred_element_type=F32)

    proj_s = lax.fori_loop(0, NC // CH, small, jnp.zeros((CZ + 16, 512), F32))

    lane128 = iota((128, 128), 1)
    sub128 = iota((128, 128), 0)
    sel_ctx = ((lane128 - 64 + 2 * head == sub128) & (lane128 >= 64) & (lane128 < 66)).astype(BF16)
    dt_ctx = bdot(proj_s[:CZ, 384:512], sel_ctx)
    lane_c = iota((CZ, 128), 1)
    cbuf[z] = jnp.concatenate([jnp.where(lane_c < 64, proj_s[:CZ, 0:128], dt_ctx), proj_s[:CZ, 128:256]], 1).astype(BF16)
    esend[0] = proj_s[CZ + 8 : CZ + 16, 0:384].astype(BF16)
    esend[1] = proj_s[CZ : CZ + 8, 0:384].astype(BF16)
    e_up = remote(esend.at[0], ebuf.at[0], es.at[0], er.at[0], {"sp": lax.rem(z + 1, Z)})
    e_down = remote(esend.at[1], ebuf.at[1], es.at[1], er.at[1], {"sp": lax.rem(z + Z - 1, Z)})
    e_up.start()
    e_down.start()

    def c_send(i, carry):
        remote(cbuf.at[z], cbuf.at[z], css, csr.at[z], {"sp": lax.rem(z + i, Z)}).start()
        return carry

    lax.fori_loop(1, Z, c_send, 0)

    acc[...] = jnp.zeros_like(acc)

    def main(i, carry):
        h, off, at = chunk(i)
        gs = gain_ref[:, pl.ds(at, KB)].astype(F32) * (1.0 + scales(i, 1))
        sh = scales(i, 0)
        v = latbuf[h, :, :, pl.ds(off, KB)].astype(F32).reshape(T, KB)
        rows = (v * r_lat * gs + sh).astype(BF16)
        acc[...] += jnp.dot(rows, wcat[pl.ds(at, KB), :], preferred_element_type=F32)
        return carry

    lax.fori_loop(0, NC // CH, main, 0)

    b0, b1 = dtb_ref[0], dtb_ref[1]
    d0, d1 = dlog_ref[0], dlog_ref[1]
    sel_col = (lane128 + 2 * head == sub128).astype(BF16) * (lane128 < 2).astype(BF16)
    sel_row = ((iota((8, 128), 0) + 2 * head == iota((8, 128), 1)) & (iota((8, 128), 0) < 2)).astype(BF16)
    dt_all = acc[:, 384:512].astype(BF16)
    nt = (((1,), (1,)), ((), ()))
    lane_t = iota((T, 128), 1)
    sub_8t = iota((8, T), 0)
    step_col = softplus(bdot(dt_all, sel_col) + jnp.where(lane_t == 0, b0, b1))
    step_row = softplus(bdot(sel_row, dt_all, nt) + jnp.where(sub_8t == 0, b0, b1))
    a_col = -step_col * jnp.exp(jnp.where(lane_t == 0, d0, d1))
    a_row = -step_row * jnp.exp(jnp.where(sub_8t == 0, d0, d1))
    q_i = iota((T, T), 0)
    s_i = iota((T, T), 1)
    low = (s_i <= q_i).astype(F32)
    upp = (s_i >= q_i).astype(F32)
    lf_col = hdot(low, a_col)[:, 0:1]
    lb_col = hdot(upp, a_col)[:, 1:2]
    lf_row = hdot(a_row, upp)[0:1]
    lb_row = hdot(a_row, low)[1:2]
    lf_tot = lf_col[T - 1 : T]
    lb_tot = lb_col[0:1]
    lane_1 = iota((1, 128), 1)
    lbuf[z] = jnp.where(lane_1 == 0, lf_tot, lb_tot)

    def l_send(i, carry):
        remote(lbuf.at[z], lbuf.at[z], ls_, lr_.at[z], {"sp": lax.rem(z + i, Z)}).start()
        return carry

    lax.fori_loop(1, Z, l_send, 0)

    e_up.wait_recv()
    e_down.wait_recv()

    def conv(v, before, after, taps, rows):
        n = v.shape[0]
        up = jnp.where(rows == 0, before, pltpu.roll(v, 1, 0))
        down = jnp.where(rows == n - 1, after, pltpu.roll(v, n - 1, 0))
        return silu(taps[0] * up + taps[1] * v + taps[2] * down)

    def taps_of(ref):
        rows = [ref[i : i + 1, :].astype(F32) for i in range(3)]
        if rows[0].shape[1] < 128:
            rows = [jnp.concatenate([r, jnp.zeros_like(r)], 1) for r in rows]
        return rows

    tx, tb, tc = taps_of(cx_ref), taps_of(cb_ref), taps_of(cc_ref)
    sub_t = iota((T, 128), 0)
    has_prev = (z > 0).astype(F32)
    has_next = (z < Z - 1).astype(F32)
    e_prev = ebuf[0].astype(F32)[7:8] * has_prev
    e_next = ebuf[1].astype(F32)[0:1] * has_next

    def seg(i):
        return acc[:, i * 128 : i * 128 + 128].astype(BF16).astype(F32)

    def edges(e, i):
        return e[:, i * 128 : i * 128 + 128]

    xz = seg(0)
    xs = conv(xz, edges(e_prev, 0), edges(e_next, 0), tx, sub_t)
    bs = conv(seg(1), edges(e_prev, 1), edges(e_next, 1), tb, sub_t)
    cs = conv(seg(2), edges(e_prev, 2), edges(e_next, 2), tc, sub_t)
    bs_b = bs.astype(BF16)
    cs_b = cs.astype(BF16)

    tn = (((0,), (0,)), ((), ()))

    def state_of(v, writes, wf, wb, lanes):
        doubled = v + pltpu.roll(v, 64, 1)
        return bdot(doubled * jnp.where(lanes < 64, wf, wb), writes, tn)

    st = state_of(
        xs, bs_b,
        jnp.exp(lf_tot - lf_col) * step_col[:, 0:1],
        jnp.exp(lb_tot - lb_col) * step_col[:, 1:2],
        lane_t,
    )
    snd[...] = st.reshape(2, 64, 128).astype(BF16)

    def s_send(i, carry):
        k = lax.rem(z + i, Z)
        back = (k < z).astype(jnp.int32)
        remote(snd.at[back], rst.at[z], sts, str_.at[z], {"sp": k}).start()
        return carry

    lax.fori_loop(1, Z, s_send, 0)

    pf = jnp.where(s_i <= q_i, jnp.exp(jnp.minimum(lf_col - lf_row, 0.0)), 0.0) * step_row[0:1]
    pb = jnp.where(s_i >= q_i, jnp.exp(jnp.minimum(lb_col - lb_row, 0.0)), 0.0) * step_row[1:2]
    inter = bdot(cs_b, bs_b, nt)
    y_in = bdot(inter * (pf + pb), xs)

    def c_wait(i, carry):
        k = lax.rem(z + i, Z)
        remote(cbuf.at[k], cbuf.at[k], css, csr.at[k], partner).wait_recv()
        return carry

    lax.fori_loop(1, Z, c_wait, 0)
    cin = cbuf[...].astype(F32).reshape(CT, 256)
    sub_c = iota((CT, 128), 0)
    lane_ct = iota((CT, 128), 1)
    zero_row = jnp.zeros((1, 128), F32)
    xs_c = conv(cin[:, 0:128], zero_row, zero_row, tx, sub_c)
    bs_c = conv(cin[:, 128:256], zero_row, zero_row, tb, sub_c)
    step_c = softplus(cin[:, 0:128] + jnp.where(lane_ct == 64, b0, b1))
    a_c = -step_c * jnp.exp(jnp.where(lane_ct == 64, d0, d1))
    q_c = iota((CT, CT), 0)
    s_c = iota((CT, CT), 1)
    cf_col = hdot((s_c <= q_c).astype(F32), a_c)[:, 64:65]
    cb_col = hdot((s_c >= q_c).astype(F32), a_c)[:, 65:66]
    cst[...] = state_of(
        xs_c, bs_c,
        jnp.exp(cf_col[CT - 1 : CT] - cf_col) * step_c[:, 64:65],
        jnp.exp(cb_col[0:1] - cb_col) * step_c[:, 65:66],
        lane_ct,
    )

    wocopy.wait_recv()

    def join_o(i, carry):
        rows = pl.ds(pl.multiple_of(i * RB, RB), RB)
        a, b = wo_own[rows, :], wo_part[rows, :]
        wo[rows, :] = jnp.where(first_core, jnp.concatenate([a, b], 1), jnp.concatenate([b, a], 1))
        return carry

    lax.fori_loop(0, D // RB, join_o, 0)

    def l_wait(i, carry):
        k = lax.rem(z + i, Z)
        remote(lbuf.at[k], lbuf.at[k], ls_, lr_.at[k], partner).wait_recv()
        remote(snd.at[0], rst.at[k], sts, str_.at[k], partner).wait_recv()
        return carry

    lax.fori_loop(1, Z, l_wait, 0)

    def enter(i, carry):
        sf, sb, runs = carry
        kf = lax.rem(z + Z - i, Z)
        kb = lax.rem(z + i, Z)
        okf = (i <= z).astype(F32)
        okb = (z + i < Z).astype(F32)
        w = jnp.exp(runs)
        sf = sf + (w[:, 0:1] * okf) * rst[kf].astype(F32)
        sb = sb + (w[:, 1:2] * okb) * rst[kb].astype(F32)
        runs = runs + jnp.where(lane_1 == 0, lbuf[kf] * okf, lbuf[kb] * okb)
        return sf, sb, runs

    zero_state = jnp.zeros((64, 128), F32)
    sf, sb, runs = lax.fori_loop(1, Z, enter, (zero_state, zero_state, jnp.zeros((1, 128), F32)))
    w = jnp.exp(runs)
    sf = sf + w[:, 0:1] * cst[0:64]
    sb = sb + w[:, 1:2] * cst[64:128]

    carried = bdot(cs_b, jnp.concatenate([sf, sb], 0), nt) * jnp.where(lane_t < 64, jnp.exp(lf_col), jnp.exp(lb_col))
    ys = y_in + carried + pltpu.roll(carried, 64, 1)
    zin = pltpu.roll(xz, 64, 1)
    g = jnp.where(lane_t < 64, ys * silu(zin), 0.0)
    hg = hg_ref[...].astype(F32)
    hg = jnp.concatenate([hg, jnp.zeros_like(hg)], 1)
    heads = g * lax.rsqrt(jnp.sum(g * g, axis=1, keepdims=True) / 64 + EPS) * hg
    heads = jnp.where(first_core, heads, pltpu.roll(heads, 64, 1))

    osend[...] = jnp.where(first_core, heads[TH:T], heads[0:TH]).astype(BF16)
    op = remote(osend, orecv, ops, opr, partner)
    op.start()
    keep = jnp.where(first_core, heads[0:TH], heads[TH:T])
    op.wait_recv()
    obuf[chip] = (keep + orecv[...].astype(F32)).astype(BF16)
    gather_open(obuf, ogs, ogr)
    gather_relay(obuf, ogs, ogr, lambda slot: None)
    gather_close(obuf, ogs, ogr, lambda slot: None)

    def out_dot(i, t):
        rows = jnp.concatenate([obuf[i * CH + j] for j in range(CH)], 1)
        return t + jnp.dot(rows, wo[pl.ds(pl.multiple_of(i * KB, KB), KB), :], preferred_element_type=F32)

    upd = lax.fori_loop(0, NC // CH, out_dot, jnp.zeros((TH, 128), F32)) * gate
    ubuf[...] = upd.reshape(TH // 8, 8, 128).astype(BF16)

    in_half = chip // HC == c

    def u_send(i, carry):
        j = lax.rem(lax.rem(head, NC) + i, NC)
        k = c * HC + j // 2
        e = lax.rem(j, 2)
        me = (k == chip) & (e == c)

        @pl.when(jnp.logical_not(me))
        def _():
            remote(
                ubuf.at[j // 2], rbuf.at[chip], us, ur.at[chip],
                {"tp_0": k // X, "tp_1": lax.rem(k, X), "tp_2": e},
            ).start()

        return carry

    lax.fori_loop(0, NC, u_send, 0)

    @pl.when(in_half)
    def _():
        rbuf[chip] = ubuf[lax.rem(chip, HC)]

    def u_wait(k, carry):
        @pl.when(jnp.logical_not(in_half & (k == chip)))
        def _():
            remote(ubuf.at[0], rbuf.at[k], us, ur.at[k], partner).wait_recv()

        return carry

    lax.fori_loop(0, NC, u_wait, 0)

    def finish(k, carry):
        cols = pl.ds(pl.multiple_of(k * 128, 128), 128)
        v = rbuf[k].astype(F32)
        v = jnp.where(first_core, v[0:4], v[4:8])
        out_ref[:, cols] = (lat_ref[:, cols].astype(F32) + v).astype(BF16)
        return carry

    lax.fori_loop(0, NC, finish, 0)

    lp.wait_send()
    mp.wait_send()
    wocopy.wait_send()
    e_up.wait_send()
    e_down.wait_send()
    op.wait_send()
    drain(mbuf.at[pl.ds(0, Z - 1)], m1s)
    drain(sbuf.at[pl.ds(0, NC - 1)], m2s)
    gather_drain(mine, lgs)
    drain(mine.at[pl.ds(0, NC)], ld_s)
    drain(cbuf.at[pl.ds(0, Z - 1)], css)
    drain(lbuf.at[pl.ds(0, Z - 1)], ls_)
    drain(rst.at[pl.ds(0, Z - 1)], sts)
    gather_drain(obuf, ogs)

    @pl.when(in_half)
    def _():
        drain(rbuf.at[pl.ds(0, NC - 1)], us)

    @pl.when(jnp.logical_not(in_half))
    def _():
        drain(rbuf.at[pl.ds(0, NC)], us)


def per_device(sizes, latent, context, cond, cond_ctx, wsh, wsc, wga, gain, pz, px, pb, pc, pdt, cx, cb, cc, dtb, dlog, hg, po):
    Z, Y, X = sizes
    NC = Y * X
    D = latent.shape[1]
    T = 8 * NC
    CZ = context.shape[0]
    if pdt.shape[1] < 128:
        pdt = jnp.pad(pdt, ((0, 0), (0, 128 - pdt.shape[1])))
    V = pltpu.VMEM
    S = pltpu.SemaphoreType.DMA
    vm = pl.BlockSpec(memory_space=pltpu.VMEM)
    hb = pl.BlockSpec(memory_space=pl.ANY)
    sm = pl.BlockSpec(memory_space=pltpu.SMEM)
    one = S
    return pl.pallas_call(
        functools.partial(kernel, sizes),
        out_shape=jax.ShapeDtypeStruct(latent.shape, BF16),
        in_specs=[vm, vm, vm, vm, vm, vm, vm, vm, hb, hb, hb, hb, hb, vm, vm, vm, sm, sm, vm, hb],
        out_specs=vm,
        scratch_shapes=[
            V((D, 512), BF16), V((D, 64), BF16), V((D, 64), BF16), V((D, 64), BF16), V((D, 64), BF16), V((D, 128), BF16),
            V((2, NC, 8, D // 2), BF16), V((4, D // 2), BF16), V((4, D // 2), BF16), V((5, 128), F32), V((5, 128), F32),
            V((Z, 5, 128), F32), V((NC, 4, 128), F32), V((T, 512), F32), V((8, 128), F32),
            V((Z, CZ, 256), BF16), V((2, 8, 384), BF16), V((2, 8, 384), BF16), V((Z, 1, 128), F32),
            V((2, 64, 128), BF16), V((Z, 64, 128), BF16), V((T // 2, 128), BF16), V((T // 2, 128), BF16),
            V((NC, T // 2, 128), BF16), V((T // 16, 8, 128), BF16), V((NC, 8, 128), BF16), V((128, 128), F32),
            S((6,)), one, one, one, one, one, one, one, S((Z,)), one, S((NC,)), one, S((NC,)), one, S((NC,)),
            one, S((Z,)), S((2,)), S((2,)), one, S((Z,)), one, S((Z,)), one, one, one, S((NC,)), one, S((NC,)),
        ],
        compiler_params=pltpu.CompilerParams(collective_id=0, has_side_effects=True, vmem_limit_bytes=48 << 20),
        name="mixer",
    )(
        latent, context, cond.reshape(1, -1), cond_ctx.reshape(1, -1), wsh, wsc, wga, gain.reshape(1, -1),
        pz, px, pb, pc, pdt, cx, cb, cc, dtb, dlog, hg.reshape(1, -1), po,
    )


def build(mesh, sizes):
    Z, Y, X = sizes
    torus = Mesh(mesh.devices.reshape(Z, Y, X, 2), SP_TP)
    in_specs = (
        P(SP_TP, None), P("sp", None), P("sp"), P("sp"), P("sp", TP), P("sp", TP), P("sp", TP), P(),
        P(None, TP), P(None, TP), P(None, TP), P(None, TP), P(), P(None, TP), P(None, TP), P(None, TP),
        P(TP), P(TP), P(TP), P(None, TP),
    )
    return jax.shard_map(
        functools.partial(per_device, sizes), mesh=torus, in_specs=in_specs, out_specs=P(SP_TP, None), check_vma=False
    )


def solution(mesh):
    return build(mesh, (mesh.shape["sp"], 8, 4))
```

```python
import functools

import jax
import jax.numpy as jnp
from jax import lax
from jax.experimental import pallas as pl
from jax.experimental.pallas import tpu as pltpu
from jax.sharding import Mesh
from jax.sharding import PartitionSpec as P

TP = ("tp_0", "tp_1", "tp_2")
SP_TP = ("sp", "tp_0", "tp_1", "tp_2")
EPS = 1e-06
MESH_ID = pl.DeviceIdType.MESH
F32 = jnp.float32
BF16 = jnp.bfloat16
HI = lax.Precision.HIGHEST


def iota(shape, dim):
    return lax.broadcasted_iota(jnp.int32, shape, dim)


def silu(v):
    return v * (1.0 / (1.0 + jnp.exp(-v)))


def softplus(v):
    return jnp.maximum(v, 0.0) + jnp.log1p(jnp.exp(-jnp.abs(v)))


def bdot(a, b, dims=(((1,), (0,)), ((), ()))):
    return lax.dot_general(a.astype(BF16), b.astype(BF16), dims, preferred_element_type=F32)


def hdot(a, b):
    return jnp.dot(a, b, precision=HI, preferred_element_type=F32)


def kernel(
    sizes,
    lat_h, ctx_h, cond_h, condc_h, wsh_h, wsc_h, wga_h, gain_h,
    pz_ref, px_ref, pb_ref, pc_ref, pdt_ref, cx_h, cb_h, cc_h, dtb_h, dlog_h, hg_h, po_ref,
    out_ref,
    lat_ref, ctx_ref, cond_ref, condc_ref, wsh_ref, wsc_ref, wga_ref, gain_ref,
    cx_ref, cb_ref, cc_ref, dtb_ref, dlog_ref, hg_ref,
    wcat, wxz, wot, wo, latbuf, pbuf, psend, mpair, mpair_r, mbuf, sbuf, acc, acco,
    cbuf, ebuf, esend, lbuf, snd, rst, osend, orecv, obuf, ubuf, rbuf, cst, ssq,
    wsem, wosem, worsem, pss, prs, mps, mpr, m1s, m1r, m2s, m2r, lgs, lgy, lgx, ld_s, ldr,
    css, csr, es, er, ls_, lr_, sts, str_, ops, opr, ogs, ogy, ogx, us, ur,
):
    Z, Y, X = sizes
    NC = Y * X
    HC = NC // 2
    D = lat_ref.shape[1]
    HD = D // 2
    HQ = D // 4
    T = NC * 8
    TH = T // 2
    CZ = ctx_ref.shape[0]
    CT = CZ * Z
    z = lax.axis_index("sp")
    y = lax.axis_index("tp_0")
    x = lax.axis_index("tp_1")
    c = lax.axis_index("tp_2")
    chip = y * X + x
    head = chip * 2 + c
    first_core = c == 0

    def remote(src, dst, ssem, rsem, dev):
        return pltpu.make_async_remote_copy(
            src_ref=src, dst_ref=dst, send_sem=ssem, recv_sem=rsem, device_id=dev, device_id_type=MESH_ID
        )

    def drain(buf, n, sem):
        if n:
            ref = buf.at[pl.ds(0, n)]
            pltpu.make_async_copy(ref, ref, sem).wait()

    partner = {"tp_2": 1 - c}

    wot_own = wot.at[pl.ds(pl.multiple_of(c * 64, 64), 64)]
    moves = [
        (lat_h, lat_ref), (wsh_h, wsh_ref), (wsc_h, wsc_ref), (wga_h, wga_ref), (cond_h, cond_ref), (condc_h, condc_ref),
        (ctx_h, ctx_ref), (gain_h, gain_ref), (cx_h, cx_ref), (cb_h, cb_ref), (cc_h, cc_ref),
        (dtb_h, dtb_ref), (dlog_h, dlog_ref), (hg_h, hg_ref),
        (po_ref, wot_own), (px_ref, wxz.at[0:64]), (pz_ref, wxz.at[64:128]),
        (pb_ref, wcat.at[:, 128:256]), (pc_ref, wcat.at[:, 256:384]), (pdt_ref, wcat.at[:, 384:512]),
    ]
    loads = [pltpu.make_async_copy(a, b, wsem.at[i]) for i, (a, b) in enumerate(moves)]
    for load in loads:
        load.start()

    bar = pltpu.get_barrier_semaphore()

    def hello(dev):
        pl.semaphore_signal(bar, inc=1, device_id=dev, device_id_type=MESH_ID)

    def greet_z(i, carry):
        hello({"sp": lax.rem(z + i, Z)})
        return carry

    def greet_row(i, carry):
        yy = lax.rem(y + i, Y)
        for d in range(X):
            xx = lax.rem(x + d, X)
            hello({"tp_0": yy, "tp_1": xx})
            hello({"tp_0": yy, "tp_1": xx, "tp_2": 1 - c})
        return carry

    hello(partner)
    for d in range(1, X):
        xx = lax.rem(x + d, X)
        hello({"tp_1": xx})
        hello({"tp_1": xx, "tp_2": 1 - c})
    lax.fori_loop(1, Y, greet_row, 0)
    lax.fori_loop(1, Z, greet_z, 0)

    nt = (((1,), (1,)), ((), ()))
    tn = (((0,), (0,)), ((), ()))

    loads[0].wait()
    lat = lat_ref[...].astype(F32)
    psend[...] = jnp.where(first_core, lat[:, HD:], lat[:, :HD]).astype(BF16)

    for load in loads[1:6]:
        load.wait()

    def line(ref):
        v = ref[...].astype(F32)
        return jnp.concatenate([v[k : k + 1] for k in range(ref.shape[0])], 1)

    row8 = iota((8, cond_ref.shape[0] * cond_ref.shape[1]), 0)
    both = jnp.where(row8 == 0, line(cond_ref), jnp.where(row8 == 1, line(condc_ref), 0.0))
    act = silu(both).astype(BF16)

    def wide(part):
        zero = jnp.zeros_like(part)
        return jnp.where(first_core, jnp.concatenate([part, zero], 1), jnp.concatenate([zero, part], 1))

    psh = wide(bdot(act, wsh_ref[...], nt))
    psc = wide(bdot(act, wsc_ref[...], nt))
    pga = wide(bdot(act, wga_ref[...], nt))
    mpair[...] = jnp.concatenate([psh[0:1], psc[0:1], psh[1:2], psc[1:2], pga[0:1]], 0)

    pl.semaphore_wait(bar, Z - 1 + NC * 2 - 1)

    lp = remote(psend, pbuf, pss, prs, partner)
    lp.start()
    mp = remote(mpair, mpair_r, mps, mpr, partner)
    mp.start()
    wocopy = remote(wot_own, wot_own, wosem, worsem, partner)

    def far_first(i):
        return Z // 2 + (1 - 2 * lax.rem(i, 2)) * ((i + 1) // 2)

    def near(n):
        return [d for k in range(1, (n + 1) // 2) for d in (k, n - k)] + ([n // 2] if n % 2 == 0 else [])

    def gather(buf, ssem, ysem, xsem, middle, row_done):
        def x_send(row):
            slot = buf.at[row * X + x]
            for d in near(X):
                remote(slot, slot, ssem, xsem.at[row], {"tp_1": lax.rem(x + d, X)}).start()

        def x_take(row):
            drain(buf, X - 1, xsem.at[row])
            row_done(row)

        own = buf.at[chip]
        x_send(y)
        for d in near(Y):
            remote(own, own, ssem, ysem.at[y], {"tp_0": lax.rem(y + d, Y)}).start()
        rows = [y]
        for n, d in enumerate(near(Y)):
            row = lax.rem(y + Y - d, Y)
            slot = buf.at[row * X + x]
            remote(slot, slot, ssem, ysem.at[row], partner).wait_recv()
            x_send(row)
            rows.append(row)
            if n in (3, 5):
                x_take(rows.pop(0))
        middle()
        for row in rows:
            x_take(row)

    mine = latbuf.at[c]
    other = latbuf.at[1 - c]

    def squares(h, row):
        for j in range(X):
            v = latbuf[h, row * X + j].astype(F32)
            v = v * v
            t = v[0] + v[1]
            ssq[h, row * X + j] = sum(t[:, k * 128 : k * 128 + 128] for k in range(HQ // 128))

    late = []

    def row_of(ref, row):
        return ref.at[pl.ds(row * X, X)]

    def from_partner():
        row = late.pop(0)
        remote(row_of(other, row), row_of(other, row), ld_s, ldr.at[row], partner).wait_recv()
        squares(1 - c, row)

    def to_partner(row):
        remote(row_of(mine, row), row_of(mine, row), ld_s, ldr.at[row], partner).start()
        squares(c, row)
        late.append(row)
        if len(late) > 2:
            from_partner()

    lp.wait_recv()
    got = pbuf[...].astype(F32)
    own = jnp.where(first_core, lat[:, :HD], lat[:, HD:])
    block = jnp.concatenate([jnp.where(first_core, own, got), jnp.where(first_core, got, own)], 0).astype(BF16)
    latbuf[c, chip, 0] = block[:, :HQ]
    latbuf[c, chip, 1] = block[:, HQ:]

    mp.wait_recv()
    mbuf[z] = mpair[...] + mpair_r[...]

    def m1_send(i, carry):
        remote(mbuf.at[z], mbuf.at[z], m1s, m1r, {"sp": lax.rem(z + far_first(i), Z)}).start()
        return carry

    lax.fori_loop(0, Z - 1, m1_send, 0)

    def m2_send(yy, xx):
        remote(sbuf.at[chip], sbuf.at[chip], m2s, m2r, {"tp_0": yy, "tp_1": xx}).start()

    def m2_row(i, carry):
        yy = lax.rem(y + i, Y)
        for d in range(X):
            m2_send(yy, lax.rem(x + d, X))
        return carry

    def modulation():
        drain(mbuf, Z - 1, m1r)
        msum = sum(mbuf[k] for k in range(Z))
        mp.wait_send()
        mpair[...] = msum
        sbuf[chip] = msum[0:4]
        lax.fori_loop(1, Y, m2_row, 0)
        for d in range(1, X):
            m2_send(y, lax.rem(x + d, X))

    scale_of = {}

    def middle():
        modulation()
        for load in loads[6:]:
            load.wait()

        def join_w(i, carry):
            span = pl.ds(pl.multiple_of(i * 128, 128), 128)
            wcat[span, 0:128] = wxz[:, span].T
            return carry

        lax.fori_loop(0, D // 128, join_w, 0)
        def sq_ctx(k, tot):
            v = ctx_ref[:, pl.ds(pl.multiple_of(k * 128, 128), 128)].astype(F32)
            return tot + v * v

        tot = lax.fori_loop(0, NC, sq_ctx, jnp.zeros((CZ, 128), F32))
        scale_of[0] = lax.rsqrt(jnp.sum(tot, axis=1, keepdims=True) / D + EPS)

        wocopy.start()

    gather(mine, lgs, lgy, lgx, middle, to_partner)
    r_ctx = scale_of[0]

    while late:
        from_partner()
    tot = (ssq[0] + ssq[1]).reshape(T, 128)
    r_lat = lax.rsqrt(jnp.sum(tot, axis=1, keepdims=True) / D + EPS)

    drain(sbuf, NC - 1, m2r)

    CH = min(4, NC // 4)
    KB = CH * 128
    NQ = HQ // KB

    def scales(i, row):
        return jnp.concatenate([sbuf[i * CH + j][row : row + 1] for j in range(CH)], 1)

    gains_all = gain_ref[...].astype(F32)

    def gains_of(i):
        return jnp.concatenate([gains_all[i * CH + j : i * CH + j + 1] for j in range(CH)], 1)

    def chunk(i):
        return i // (2 * NQ), i // NQ % 2, i % NQ * KB, i * KB

    def small(i, carry):
        h, q, off, at = chunk(i)
        gains = gains_of(i)
        gs = gains * (1.0 + scales(i, 1))
        sh = scales(i, 0)
        gsc = gains * (1.0 + scales(i, 3))
        shc = scales(i, 2)
        vc = ctx_ref[:, pl.ds(at, KB)].astype(F32) * r_ctx * gsc + shc
        v0 = latbuf[h, 0, q, :, pl.ds(off, KB)].astype(F32) * r_lat[0:8] * gs + sh
        v1 = latbuf[h, NC - 1, q, :, pl.ds(off, KB)].astype(F32) * r_lat[T - 8 : T] * gs + sh
        rows = jnp.concatenate([vc, v0, v1], 0).astype(BF16)
        return carry + jnp.dot(rows, wcat[pl.ds(at, KB), :], preferred_element_type=F32)

    proj_s = jnp.zeros((CZ + 16, 512), F32)
    for i in range(NC // CH):
        proj_s = small(i, proj_s)

    lane128 = iota((128, 128), 1)
    sub128 = iota((128, 128), 0)
    sel_ctx = ((lane128 - 64 + 2 * head == sub128) & (lane128 >= 64) & (lane128 < 66)).astype(BF16)
    dt_ctx = bdot(proj_s[:CZ, 384:512], sel_ctx)
    lane_c = iota((CZ, 128), 1)
    cbuf[z] = jnp.concatenate([jnp.where(lane_c < 64, proj_s[:CZ, 0:128], dt_ctx), proj_s[:CZ, 128:256]], 1).astype(BF16)
    esend[0] = proj_s[CZ + 8 : CZ + 16, 0:384].astype(BF16)
    esend[1] = proj_s[CZ : CZ + 8, 0:384].astype(BF16)
    e_up = remote(esend.at[0], ebuf.at[0], es.at[0], er.at[0], {"sp": lax.rem(z + 1, Z)})
    e_down = remote(esend.at[1], ebuf.at[1], es.at[1], er.at[1], {"sp": lax.rem(z + Z - 1, Z)})
    e_up.start()
    e_down.start()

    c_first = remote(cbuf.at[z], cbuf.at[z], css.at[0], csr, {"sp": jnp.int32(0)})
    c_last = remote(cbuf.at[z], cbuf.at[z], css.at[1], csr, {"sp": jnp.int32(Z - 1)})

    @pl.when(z > 0)
    def _():
        c_first.start()

    @pl.when(z < Z - 1)
    def _():
        c_last.start()

    def main(i, total):
        h, q, off, at = chunk(i)
        gs = gains_of(i) * (1.0 + scales(i, 1))
        sh = scales(i, 0)
        v = latbuf[h, :, q, :, pl.ds(off, KB)].astype(F32).reshape(T, KB)
        rows = (v * r_lat * gs + sh).astype(BF16)
        return total + jnp.dot(rows, wcat[pl.ds(at, KB), :], preferred_element_type=F32)

    total = jnp.zeros((T, 512), F32)
    for i in range(NC // CH):
        total = main(i, total)
    acc[...] = total

    b0, b1 = dtb_ref[:, 0:1], dtb_ref[:, 1:2]
    d0, d1 = dlog_ref[:, 0:1], dlog_ref[:, 1:2]
    sel_col = (lane128 + 2 * head == sub128).astype(BF16) * (lane128 < 2).astype(BF16)
    sel_row = ((iota((8, 128), 0) + 2 * head == iota((8, 128), 1)) & (iota((8, 128), 0) < 2)).astype(BF16)
    dt_all = acc[:, 384:512].astype(BF16)
    lane_t = iota((T, 128), 1)
    sub_8t = iota((8, T), 0)
    step_col = softplus(bdot(dt_all, sel_col) + jnp.where(lane_t == 0, b0, b1))
    step_row = softplus(bdot(sel_row, dt_all, nt) + jnp.where(sub_8t == 0, b0, b1))
    a_col = -step_col * jnp.exp(jnp.where(lane_t == 0, d0, d1))
    a_row = -step_row * jnp.exp(jnp.where(sub_8t == 0, d0, d1))
    q_i = iota((T, T), 0)
    s_i = iota((T, T), 1)
    low = (s_i <= q_i).astype(BF16)
    upp = (s_i >= q_i).astype(BF16)

    def split(v):
        hi = v.astype(BF16)
        rest = v - hi.astype(F32)
        mid = rest.astype(BF16)
        return hi, mid, (rest - mid.astype(F32)).astype(BF16)

    def sums_down(mask, v):
        return sum(jnp.dot(mask, p, preferred_element_type=F32) for p in split(v))

    cum_col = sums_down(low, a_col)
    cum_row = sum(jnp.dot(p, upp, preferred_element_type=F32) for p in split(a_row))
    lf_col = cum_col[:, 0:1]
    lf_tot = cum_col[T - 1 : T, 0:1]
    lb_tot = cum_col[T - 1 : T, 1:2]
    lb_col = lb_tot - cum_col[:, 1:2] + a_col[:, 1:2]
    lf_row = cum_row[0:1]
    lb_row = lb_tot - cum_row[1:2] + a_row[1:2]
    lane_1 = iota((1, 128), 1)
    lbuf[z] = jnp.where(lane_1 == 0, lf_tot, lb_tot)

    def l_send(i, carry):
        remote(lbuf.at[z], lbuf.at[z], ls_, lr_, {"sp": lax.rem(z + far_first(i), Z)}).start()
        return carry

    lax.fori_loop(0, Z - 1, l_send, 0)

    e_up.wait_recv()
    e_down.wait_recv()

    def conv(v, before, after, taps, rows):
        n = v.shape[0]
        up = jnp.where(rows == 0, before, pltpu.roll(v, 1, 0))
        down = jnp.where(rows == n - 1, after, pltpu.roll(v, n - 1, 0))
        return silu(taps[0] * up + taps[1] * v + taps[2] * down)

    def taps_of(ref):
        rows = [ref[i : i + 1, :].astype(F32) for i in range(3)]
        if rows[0].shape[1] < 128:
            rows = [jnp.concatenate([r, jnp.zeros_like(r)], 1) for r in rows]
        return rows

    tx, tb, tc = taps_of(cx_ref), taps_of(cb_ref), taps_of(cc_ref)
    sub_t = iota((T, 128), 0)
    has_prev = (z > 0).astype(F32)
    has_next = (z < Z - 1).astype(F32)
    e_prev = ebuf[0].astype(F32)[7:8] * has_prev
    e_next = ebuf[1].astype(F32)[0:1] * has_next

    def seg(i):
        return acc[:, i * 128 : i * 128 + 128].astype(BF16).astype(F32)

    def edges(e, i):
        return e[:, i * 128 : i * 128 + 128]

    xz = seg(0)
    xs = conv(xz, edges(e_prev, 0), edges(e_next, 0), tx, sub_t)
    bs = conv(seg(1), edges(e_prev, 1), edges(e_next, 1), tb, sub_t)
    cs = conv(seg(2), edges(e_prev, 2), edges(e_next, 2), tc, sub_t)
    bs_b = bs.astype(BF16)
    cs_b = cs.astype(BF16)


    def state_of(v, writes, wf, wb, lanes):
        doubled = v + pltpu.roll(v, 64, 1)
        return bdot(doubled * jnp.where(lanes < 64, wf, wb), writes, tn)

    st = state_of(
        xs, bs_b,
        jnp.exp(lf_tot - lf_col) * step_col[:, 0:1],
        jnp.exp(lb_tot - lb_col) * step_col[:, 1:2],
        lane_t,
    )
    snd[...] = st.reshape(2, 64, 128).astype(BF16)
    cst[...] = jnp.zeros_like(cst)

    @pl.when((z == 0) | (z == Z - 1))
    def _():
        drain(cbuf, Z - 1, csr)
        cin = cbuf[...].astype(F32).reshape(CT, 256)
        sub_c = iota((CT, 128), 0)
        lane_ct = iota((CT, 128), 1)
        zero_row = jnp.zeros((1, 128), F32)
        xs_c = conv(cin[:, 0:128], zero_row, zero_row, tx, sub_c)
        bs_c = conv(cin[:, 128:256], zero_row, zero_row, tb, sub_c)
        step_c = softplus(cin[:, 0:128] + jnp.where(lane_ct == 64, b0, b1))
        a_c = -step_c * jnp.exp(jnp.where(lane_ct == 64, d0, d1))
        q_c = iota((CT, CT), 0)
        s_c = iota((CT, CT), 1)
        cf_col = sums_down((s_c <= q_c).astype(BF16), a_c)[:, 64:65]
        cb_col = sums_down((s_c >= q_c).astype(BF16), a_c)[:, 65:66]
        states = state_of(
            xs_c, bs_c,
            jnp.exp(cf_col[CT - 1 : CT] - cf_col) * step_c[:, 64:65],
            jnp.exp(cb_col[0:1] - cb_col) * step_c[:, 65:66],
            lane_ct,
        )
        cst[...] = states
        snd[...] = (st + states * jnp.where(sub128 < 64, jnp.exp(lf_tot), jnp.exp(lb_tot))).reshape(2, 64, 128).astype(BF16)

    def s_send(i, carry):
        k = lax.rem(z + far_first(i), Z)
        back = (k < z).astype(jnp.int32)
        remote(snd.at[back], rst.at[z], sts, str_, {"sp": k}).start()
        return carry

    lax.fori_loop(0, Z - 1, s_send, 0)

    pf = jnp.where(s_i <= q_i, jnp.exp(jnp.minimum(lf_col - lf_row, 0.0)), 0.0) * step_row[0:1]
    pb = jnp.where(s_i >= q_i, jnp.exp(jnp.minimum(lb_col - lb_row, 0.0)), 0.0) * step_row[1:2]
    inter = bdot(cs_b, bs_b, nt)
    y_in = bdot(inter * (pf + pb), xs)

    wocopy.wait_recv()

    def join_o(i, carry):
        span = pl.ds(pl.multiple_of(i * 128, 128), 128)
        wo[span, :] = wot[:, span].T
        return carry

    lax.fori_loop(0, D // 128, join_o, 0)

    drain(lbuf, Z - 1, lr_)
    drain(rst, Z - 1, str_)

    sf = cst[0:64] * (z == 0).astype(F32)
    sb = cst[64:128] * (z == Z - 1).astype(F32)
    runs = jnp.zeros((1, 128), F32)
    for i in range(1, Z):
        kf = lax.rem(z + Z - i, Z)
        kb = lax.rem(z + i, Z)
        okf = (i <= z).astype(F32)
        okb = (z + i < Z).astype(F32)
        w = jnp.exp(runs)
        sf = sf + (w[:, 0:1] * okf) * rst[kf].astype(F32)
        sb = sb + (w[:, 1:2] * okb) * rst[kb].astype(F32)
        runs = runs + jnp.where(lane_1 == 0, lbuf[kf] * okf, lbuf[kb] * okb)

    carried = bdot(cs_b, jnp.concatenate([sf, sb], 0), nt) * jnp.where(lane_t < 64, jnp.exp(lf_col), jnp.exp(lb_col))
    ys = y_in + carried + pltpu.roll(carried, 64, 1)
    zin = pltpu.roll(xz, 64, 1)
    g = jnp.where(lane_t < 64, ys * silu(zin), 0.0)
    hg = hg_ref[...].astype(F32)
    hg = jnp.concatenate([hg, jnp.zeros_like(hg)], 1)
    heads = g * lax.rsqrt(jnp.sum(g * g, axis=1, keepdims=True) / 64 + EPS) * hg
    heads = jnp.where(first_core, heads, pltpu.roll(heads, 64, 1))

    osend[...] = jnp.where(first_core, heads[TH:T], heads[0:TH]).astype(BF16)
    op = remote(osend, orecv, ops, opr, partner)
    op.start()
    keep = jnp.where(first_core, heads[0:TH], heads[TH:T])
    op.wait_recv()
    joined = (keep + orecv[...].astype(F32)).astype(BF16)
    obuf[chip] = joined
    acco[...] = jnp.zeros_like(acco)

    def row_dot(row):
        rows = jnp.concatenate([obuf[row * X + j] for j in range(X)], 1)
        span = pl.ds(pl.multiple_of(row * (X * 128), 128), X * 128)
        acco[...] += jnp.dot(rows, wo[span, :], preferred_element_type=F32)

    gather(obuf, ogs, ogy, ogx, lambda: None, row_dot)
    upd = acco[...] * mpair[4:5]
    ubuf[...] = upd.reshape(TH // 8, 8, 128).astype(BF16)

    in_half = chip // HC == c

    def u_row(i, carry):
        r = lax.rem(lax.rem(y, Y // 2) + i, Y // 2)
        yy = c * (Y // 2) + r
        for d in range(X):
            xx = lax.rem(x + d, X)
            for e in range(2):
                copy = remote(
                    ubuf.at[r * X + xx], rbuf.at[chip], us, ur,
                    {"tp_0": yy, "tp_1": xx, "tp_2": c if e == 0 else 1 - c},
                )
                if d == 0 and e == 0:

                    @pl.when(yy != y)
                    def _():
                        copy.start()
                else:
                    copy.start()
        return carry

    lax.fori_loop(0, Y // 2, u_row, 0)

    @pl.when(in_half)
    def _():
        rbuf[chip] = ubuf[lax.rem(chip, HC)]

    @pl.when(in_half)
    def _():
        drain(rbuf, NC - 1, ur)

    @pl.when(jnp.logical_not(in_half))
    def _():
        drain(rbuf, NC, ur)

    def finish(k, carry):
        cols = pl.ds(pl.multiple_of(k * 128, 128), 128)
        v = rbuf[k].astype(F32)
        v = jnp.where(first_core, v[0:4], v[4:8])
        out_ref[:, cols] = (lat_ref[:, cols].astype(F32) + v).astype(BF16)
        return carry

    lax.fori_loop(0, NC, finish, 0)

    lp.wait_send()
    wocopy.wait_send()
    e_up.wait_send()
    e_down.wait_send()
    op.wait_send()
    drain(mbuf, Z - 1, m1s)
    drain(sbuf, NC - 1, m2s)
    drain(mine, NC - 1, lgs)
    drain(mine, NC, ld_s)

    @pl.when(z > 0)
    def _():
        c_first.wait_send()

    @pl.when(z < Z - 1)
    def _():
        c_last.wait_send()

    drain(lbuf, Z - 1, ls_)
    drain(rst, Z - 1, sts)
    drain(obuf, NC - 1, ogs)

    @pl.when(in_half)
    def _():
        drain(rbuf, NC - 1, us)

    @pl.when(jnp.logical_not(in_half))
    def _():
        drain(rbuf, NC, us)


def per_device(sizes, latent, context, cond, cond_ctx, wsh, wsc, wga, gain, pz, px, pb, pc, pdt, cx, cb, cc, dtb, dlog, hg, po):
    Z, Y, X = sizes
    NC = Y * X
    D = latent.shape[1]
    T = 8 * NC
    CZ = context.shape[0]
    if pdt.shape[1] < 128:
        pdt = jnp.pad(pdt, ((0, 0), (0, 128 - pdt.shape[1])))
    V = pltpu.VMEM

    def lines(v):
        return (v.size // 128, 128)

    S = pltpu.SemaphoreType.DMA
    vm = pl.BlockSpec(memory_space=pltpu.VMEM)
    hb = pl.BlockSpec(memory_space=pl.ANY)
    one = S
    return pl.pallas_call(
        functools.partial(kernel, sizes),
        out_shape=jax.ShapeDtypeStruct(latent.shape, BF16),
        in_specs=[hb] * 20,
        out_specs=vm,
        scratch_shapes=[
            V((4, D), BF16), V((CZ, D), BF16), V(lines(cond), BF16), V(lines(cond), BF16),
            V((64, D // Z), BF16), V((64, D // Z), BF16), V((64, D // Z), BF16), V(lines(gain), BF16),
            V((3, 64), BF16), V((3, 128), BF16), V((3, 128), BF16), V((1, 2), F32), V((1, 2), F32), V((1, 64), BF16),
            V((D, 512), BF16), V((128, D), BF16), V((128, D), BF16), V((D, 128), BF16),
            V((2, NC, 2, 8, D // 4), BF16), V((4, D // 2), BF16), V((4, D // 2), BF16), V((5, 128), F32), V((5, 128), F32),
            V((Z, 5, 128), F32), V((NC, 4, 128), F32), V((T, 512), F32), V((T // 2, 128), F32),
            V((Z, CZ, 256), BF16), V((2, 8, 384), BF16), V((2, 8, 384), BF16), V((Z, 1, 128), F32),
            V((2, 64, 128), BF16), V((Z, 64, 128), BF16), V((T // 2, 128), BF16), V((T // 2, 128), BF16),
            V((NC, T // 2, 128), BF16), V((T // 16, 8, 128), BF16), V((NC, 8, 128), BF16), V((128, 128), F32), V((2, NC, 8, 128), F32),
            S((20,)), one, one, one, one, one, one, one, one, one, one, one, S((Y,)), S((Y,)), one, S((Y,)),
            S((2,)), one, S((2,)), S((2,)), one, one, one, one, one, one, one, S((Y,)), S((Y,)), one, one,
        ],
        compiler_params=pltpu.CompilerParams(collective_id=0, has_side_effects=True),
        name="mixer",
    )(
        latent, context, cond.reshape(lines(cond)), cond_ctx.reshape(lines(cond)), wsh.T, wsc.T, wga.T, gain.reshape(lines(gain)),
        pz.T, px.T, pb, pc, pdt, cx, cb, cc, dtb.reshape(1, 2), dlog.reshape(1, 2), hg.reshape(1, -1), po.T,
    )


def build(mesh, sizes):
    Z, Y, X = sizes
    torus = Mesh(mesh.devices.reshape(Z, Y, X, 2), SP_TP)
    in_specs = (
        P(SP_TP, None), P("sp", None), P("sp"), P("sp"), P("sp", TP), P("sp", TP), P("sp", TP), P(),
        P(None, TP), P(None, TP), P(None, TP), P(None, TP), P(), P(None, TP), P(None, TP), P(None, TP),
        P(TP), P(TP), P(TP), P(None, TP),
    )
    return jax.shard_map(
        functools.partial(per_device, sizes), mesh=torus, in_specs=in_specs, out_specs=P(SP_TP, None), check_vma=False
    )


def solution(mesh):
    return build(mesh, (mesh.shape["sp"], 8, 4))
```

```python
import functools

import jax
import jax.numpy as jnp
from jax import lax
from jax.experimental import pallas as pl
from jax.experimental.pallas import tpu as pltpu
from jax.sharding import Mesh
from jax.sharding import PartitionSpec as P

TP = ("tp_0", "tp_1", "tp_2")
SP_TP = ("sp", "tp_0", "tp_1", "tp_2")
EPS = 1e-06
MESH_ID = pl.DeviceIdType.MESH
F32 = jnp.float32
BF16 = jnp.bfloat16
HI = lax.Precision.HIGHEST


def iota(shape, dim):
    return lax.broadcasted_iota(jnp.int32, shape, dim)


def silu(v):
    return v * (1.0 / (1.0 + jnp.exp(-v)))


def softplus(v):
    return jnp.maximum(v, 0.0) + jnp.log1p(jnp.exp(-jnp.abs(v)))


def bdot(a, b, dims=(((1,), (0,)), ((), ()))):
    return lax.dot_general(a.astype(BF16), b.astype(BF16), dims, preferred_element_type=F32)


def hdot(a, b):
    return jnp.dot(a, b, precision=HI, preferred_element_type=F32)


def kernel(
    sizes,
    lat_h, ctx_h, cond_h, condc_h, wsh_h, wsc_h, wga_h, gain_h,
    pz_ref, px_ref, pb_ref, pc_ref, pdt_ref, cx_h, cb_h, cc_h, dtb_h, dlog_h, hg_h, po_ref,
    out_ref,
    lat_ref, ctx_ref, cond_ref, condc_ref, wsh_ref, wsc_ref, wga_ref, gain_ref,
    cx_ref, cb_ref, cc_ref, dtb_ref, dlog_ref, hg_ref,
    wcat, wxz, wot, wo, latbuf, pbuf, psend, mpair, mpair_r, mbuf, sbuf, acc, acco,
    cbuf, ebuf, esend, lbuf, snd, rst, osend, orecv, obuf, ubuf, rbuf, cst, ssq,
    wsem, wosem, worsem, pss, prs, mps, mpr, m1s, m1r, m2s, m2r, lgs, lgy, lgx, lga, lgb, ld_s, ldr, lda,
    css, csr, es, er, ls_, lr_, sts, str_, ops, opr, ogs, ogy, ogx, oga, ogb, us, ur,
):
    Z, Y, X = sizes
    NC = Y * X
    HC = NC // 2
    D = lat_ref.shape[1]
    HD = D // 2
    LT = HD // 128
    T = NC * 8
    TH = T // 2
    CZ = ctx_ref.shape[0]
    CT = CZ * Z
    z = lax.axis_index("sp")
    y = lax.axis_index("tp_0")
    x = lax.axis_index("tp_1")
    c = lax.axis_index("tp_2")
    chip = y * X + x
    head = chip * 2 + c
    first_core = c == 0

    def remote(src, dst, ssem, rsem, dev):
        return pltpu.make_async_remote_copy(
            src_ref=src, dst_ref=dst, send_sem=ssem, recv_sem=rsem, device_id=dev, device_id_type=MESH_ID
        )

    def drain(buf, n, sem):
        if n:
            ref = buf.at[pl.ds(0, n)]
            pltpu.make_async_copy(ref, ref, sem).wait()

    partner = {"tp_2": 1 - c}

    bar = pltpu.get_barrier_semaphore()

    def hello(dev):
        pl.semaphore_signal(bar, inc=1, device_id=dev, device_id_type=MESH_ID)

    def greet_z(i, carry):
        hello({"sp": lax.rem(z + i, Z)})
        return carry

    def greet_row(i, carry):
        yy = lax.rem(y + i, Y)
        for d in range(X):
            xx = lax.rem(x + d, X)
            hello({"tp_0": yy, "tp_1": xx})
            hello({"tp_0": yy, "tp_1": xx, "tp_2": 1 - c})
        return carry

    lax.fori_loop(1, Z, greet_z, 0)
    hello(partner)
    for d in range(1, X):
        xx = lax.rem(x + d, X)
        hello({"tp_1": xx})
        hello({"tp_1": xx, "tp_2": 1 - c})
    lax.fori_loop(1, Y, greet_row, 0)

    wot_own = wot.at[pl.ds(pl.multiple_of(c * 64, 64), 64)]
    moves = [
        (lat_h, lat_ref), (wsh_h, wsh_ref), (wsc_h, wsc_ref), (wga_h, wga_ref), (cond_h, cond_ref), (condc_h, condc_ref),
        (ctx_h, ctx_ref), (gain_h, gain_ref), (cx_h, cx_ref), (cb_h, cb_ref), (cc_h, cc_ref),
        (dtb_h, dtb_ref), (dlog_h, dlog_ref), (hg_h, hg_ref),
        (po_ref, wot_own), (px_ref, wxz.at[0:64]), (pz_ref, wxz.at[64:128]),
        (pb_ref, wcat.at[:, 128:256]), (pc_ref, wcat.at[:, 256:384]), (pdt_ref, wcat.at[:, 384:512]),
    ]
    loads = [pltpu.make_async_copy(a, b, wsem.at[i]) for i, (a, b) in enumerate(moves)]
    for load in loads:
        load.start()

    nt = (((1,), (1,)), ((), ()))
    tn = (((0,), (0,)), ((), ()))

    loads[0].wait()
    lat = lat_ref[...].astype(F32)
    psend[...] = jnp.where(first_core, lat[:, HD:], lat[:, :HD]).astype(BF16)

    for load in loads[1:6]:
        load.wait()

    def line(ref):
        v = ref[...].astype(F32)
        return jnp.concatenate([v[k : k + 1] for k in range(ref.shape[0])], 1)

    row8 = iota((8, cond_ref.shape[0] * cond_ref.shape[1]), 0)
    both = jnp.where(row8 == 0, line(cond_ref), jnp.where(row8 == 1, line(condc_ref), 0.0))
    act = silu(both).astype(BF16)

    def wide(part):
        zero = jnp.zeros_like(part)
        return jnp.where(first_core, jnp.concatenate([part, zero], 1), jnp.concatenate([zero, part], 1))

    psh = wide(bdot(act, wsh_ref[...], nt))
    psc = wide(bdot(act, wsc_ref[...], nt))
    pga = wide(bdot(act, wga_ref[...], nt))
    mpair[...] = jnp.concatenate([psh[0:1], psc[0:1], psh[1:2], psc[1:2], pga[0:1]], 0)

    pl.semaphore_wait(bar, Z - 1 + NC * 2 - 1)

    lp = remote(psend, pbuf, pss, prs, partner)
    lp.start()
    mp = remote(mpair, mpair_r, mps, mpr, partner)
    mp.start()
    wocopy = remote(wot_own, wot_own, wosem, worsem, partner)

    def far_first(i):
        return Z // 2 + (1 - 2 * lax.rem(i, 2)) * ((i + 1) // 2)

    def near(n):
        return [d for k in range(1, (n + 1) // 2) for d in (k, n - k)] + ([n // 2] if n % 2 == 0 else [])

    def groups(buf):
        n = buf.shape[1]
        few = max(1, n // 8)
        return n - few, few

    def gather(buf, ssem, ysem, xsem, asem, bsem, middle, row_done):
        nb, na = groups(buf)

        def copy(k, part, sem, dev):
            ref = buf.at[k, pl.ds(0, nb)] if part == 0 else buf.at[k, pl.ds(nb, na)]
            return remote(ref, ref, ssem, sem, dev)

        def along_x(row, part, sem_of):
            for d in near(X):
                copy(row * X + x, part, sem_of, {"tp_1": lax.rem(x + d, X)}).start()

        def along_y(col, part, sem_of):
            for d in near(Y):
                copy(y * X + col, part, sem_of, {"tp_0": lax.rem(y + d, Y)}).start()

        def x_take(row):
            ref = buf.at[pl.ds(0, X - 1), pl.ds(0, nb)]
            pltpu.make_async_copy(ref, ref, xsem.at[row]).wait()
            row_done(row)

        cols = [lax.rem(x + X - d, X) for d in near(X)]

        def turn():
            col = cols.pop(0)
            copy(y * X + col, 1, asem.at[col], partner).wait_recv()
            along_y(col, 1, bsem)

        along_x(y, 1, asem.at[x])
        along_y(x, 0, ysem.at[y])
        along_x(y, 0, xsem.at[y])
        along_y(x, 1, bsem)
        rows = [y]
        for n, d in enumerate(near(Y)):
            row = lax.rem(y + Y - d, Y)
            copy(row * X + x, 0, ysem.at[row], partner).wait_recv()
            along_x(row, 0, xsem.at[row])
            rows.append(row)
            if n == 1:
                while len(cols) > 1:
                    turn()
            if n == 3:
                while cols:
                    turn()
            if n in (3, 5):
                x_take(rows.pop(0))
        while cols:
            turn()
        middle()
        for row in rows:
            x_take(row)
        ref = buf.at[pl.ds(0, NC - X), pl.ds(0, na)]
        pltpu.make_async_copy(ref, ref, bsem).wait()

    def gather_drain(buf, sem):
        drain(buf, NC - 1, sem)

    mine = latbuf.at[c]
    other = latbuf.at[1 - c]

    nb_lat, na_lat = groups(mine)

    def squares(h, row):
        for j in range(X):
            v = latbuf[h, row * X + j, 0:nb_lat].astype(F32)
            ssq[h, row * X + j] = jnp.sum(v * v, axis=0)

    def squares_last(h):
        total = ssq[h]
        for k in range(na_lat):
            v = latbuf[h, :, nb_lat + k].astype(F32)
            total = total + v * v
        return total

    late = []

    def row_of(ref, row):
        return ref.at[pl.ds(row * X, X), pl.ds(0, nb_lat)]

    def last_of(ref):
        return ref.at[pl.ds(0, NC), pl.ds(nb_lat, na_lat)]

    def from_partner():
        row = late.pop(0)
        remote(row_of(other, row), row_of(other, row), ld_s, ldr.at[row], partner).wait_recv()
        squares(1 - c, row)

    def to_partner(row):
        remote(row_of(mine, row), row_of(mine, row), ld_s, ldr.at[row], partner).start()
        squares(c, row)
        late.append(row)
        if len(late) > 2:
            from_partner()

    lp.wait_recv()
    got = pbuf[...].astype(F32)
    own = jnp.where(first_core, lat[:, :HD], lat[:, HD:])
    block = jnp.concatenate([jnp.where(first_core, own, got), jnp.where(first_core, got, own)], 0).astype(BF16)
    for k in range(LT):
        latbuf[c, chip, k] = block[:, k * 128 : k * 128 + 128]

    mp.wait_recv()
    mbuf[z] = mpair[...] + mpair_r[...]

    def m1_send(i, carry):
        remote(mbuf.at[z], mbuf.at[z], m1s, m1r, {"sp": lax.rem(z + far_first(i), Z)}).start()
        return carry

    lax.fori_loop(0, Z - 1, m1_send, 0)

    def m2_send(yy, xx):
        remote(sbuf.at[chip], sbuf.at[chip], m2s, m2r, {"tp_0": yy, "tp_1": xx}).start()

    def m2_row(i, carry):
        yy = lax.rem(y + i, Y)
        for d in range(X):
            m2_send(yy, lax.rem(x + d, X))
        return carry

    def modulation():
        drain(mbuf, Z - 1, m1r)
        msum = sum(mbuf[k] for k in range(Z))
        mp.wait_send()
        mpair[...] = msum
        sbuf[chip] = msum[0:4]
        lax.fori_loop(1, Y, m2_row, 0)
        for d in range(1, X):
            m2_send(y, lax.rem(x + d, X))

    scale_of = {}

    def middle():
        modulation()
        for load in loads[6:]:
            load.wait()

        def join_w(i, carry):
            span = pl.ds(pl.multiple_of(i * 128, 128), 128)
            wcat[span, 0:128] = wxz[:, span].T
            return carry

        lax.fori_loop(0, D // 128, join_w, 0)
        def sq_ctx(k, tot):
            v = ctx_ref[:, pl.ds(pl.multiple_of(k * 128, 128), 128)].astype(F32)
            return tot + v * v

        tot = lax.fori_loop(0, NC, sq_ctx, jnp.zeros((CZ, 128), F32))
        scale_of[0] = lax.rsqrt(jnp.sum(tot, axis=1, keepdims=True) / D + EPS)

        wocopy.start()

    gather(mine, lgs, lgy, lgx, lga, lgb, middle, to_partner)
    last = remote(last_of(mine), last_of(mine), ld_s, lda, partner)
    last.start()
    r_ctx = scale_of[0]

    while late:
        from_partner()
    own_squares = squares_last(c)
    last.wait_recv()
    tot = (own_squares + squares_last(1 - c)).reshape(T, 128)
    r_lat = lax.rsqrt(jnp.sum(tot, axis=1, keepdims=True) / D + EPS)

    drain(sbuf, NC - 1, m2r)

    CH = min(4, HC)
    KB = CH * 128
    NQ = HD // KB

    def scales(i, row):
        return jnp.concatenate([sbuf[i * CH + j][row : row + 1] for j in range(CH)], 1)

    gains_all = gain_ref[...].astype(F32)

    def gains_of(i):
        return jnp.concatenate([gains_all[i * CH + j : i * CH + j + 1] for j in range(CH)], 1)

    def chunk(i):
        return i // NQ, i % NQ * CH, i * KB

    def tiles(h, slot, k):
        return jnp.concatenate([latbuf[h, slot, k + j].astype(F32) for j in range(CH)], 1)

    def small(i, carry):
        h, k, at = chunk(i)
        gains = gains_of(i)
        gs = gains * (1.0 + scales(i, 1))
        sh = scales(i, 0)
        gsc = gains * (1.0 + scales(i, 3))
        shc = scales(i, 2)
        vc = ctx_ref[:, pl.ds(at, KB)].astype(F32) * r_ctx * gsc + shc
        v0 = tiles(h, 0, k) * r_lat[0:8] * gs + sh
        v1 = tiles(h, NC - 1, k) * r_lat[T - 8 : T] * gs + sh
        rows = jnp.concatenate([vc, v0, v1], 0).astype(BF16)
        return carry + jnp.dot(rows, wcat[pl.ds(at, KB), :], preferred_element_type=F32)

    proj_s = jnp.zeros((CZ + 16, 512), F32)
    for i in range(NC // CH):
        proj_s = small(i, proj_s)

    lane128 = iota((128, 128), 1)
    sub128 = iota((128, 128), 0)
    sel_ctx = ((lane128 - 64 + 2 * head == sub128) & (lane128 >= 64) & (lane128 < 66)).astype(BF16)
    dt_ctx = bdot(proj_s[:CZ, 384:512], sel_ctx)
    lane_c = iota((CZ, 128), 1)
    cbuf[z] = jnp.concatenate([jnp.where(lane_c < 64, proj_s[:CZ, 0:128], dt_ctx), proj_s[:CZ, 128:256]], 1).astype(BF16)
    esend[0] = proj_s[CZ + 8 : CZ + 16, 0:384].astype(BF16)
    esend[1] = proj_s[CZ : CZ + 8, 0:384].astype(BF16)
    e_up = remote(esend.at[0], ebuf.at[0], es.at[0], er.at[0], {"sp": lax.rem(z + 1, Z)})
    e_down = remote(esend.at[1], ebuf.at[1], es.at[1], er.at[1], {"sp": lax.rem(z + Z - 1, Z)})
    e_up.start()
    e_down.start()

    c_first = remote(cbuf.at[z], cbuf.at[z], css.at[0], csr, {"sp": jnp.int32(0)})
    c_last = remote(cbuf.at[z], cbuf.at[z], css.at[1], csr, {"sp": jnp.int32(Z - 1)})

    @pl.when(z > 0)
    def _():
        c_first.start()

    @pl.when(z < Z - 1)
    def _():
        c_last.start()

    def main(i, total):
        h, k, at = chunk(i)
        gs = gains_of(i) * (1.0 + scales(i, 1))
        sh = scales(i, 0)
        v = jnp.concatenate([latbuf[h, :, k + j].astype(F32).reshape(T, 128) for j in range(CH)], 1)
        rows = (v * r_lat * gs + sh).astype(BF16)
        return total + jnp.dot(rows, wcat[pl.ds(at, KB), :], preferred_element_type=F32)

    total = jnp.zeros((T, 512), F32)
    for i in range(NC // CH):
        total = main(i, total)
    acc[...] = total

    b0, b1 = dtb_ref[:, 0:1], dtb_ref[:, 1:2]
    d0, d1 = dlog_ref[:, 0:1], dlog_ref[:, 1:2]
    sel_col = (lane128 + 2 * head == sub128).astype(BF16) * (lane128 < 2).astype(BF16)
    sel_row = ((iota((8, 128), 0) + 2 * head == iota((8, 128), 1)) & (iota((8, 128), 0) < 2)).astype(BF16)
    dt_all = acc[:, 384:512].astype(BF16)
    lane_t = iota((T, 128), 1)
    sub_8t = iota((8, T), 0)
    step_col = softplus(bdot(dt_all, sel_col) + jnp.where(lane_t == 0, b0, b1))
    step_row = softplus(bdot(sel_row, dt_all, nt) + jnp.where(sub_8t == 0, b0, b1))
    a_col = -step_col * jnp.exp(jnp.where(lane_t == 0, d0, d1))
    a_row = -step_row * jnp.exp(jnp.where(sub_8t == 0, d0, d1))
    q_i = iota((T, T), 0)
    s_i = iota((T, T), 1)
    low = (s_i <= q_i).astype(BF16)
    upp = (s_i >= q_i).astype(BF16)

    def split(v):
        hi = v.astype(BF16)
        rest = v - hi.astype(F32)
        mid = rest.astype(BF16)
        return hi, mid, (rest - mid.astype(F32)).astype(BF16)

    def sums_down(mask, v):
        return sum(jnp.dot(mask, p, preferred_element_type=F32) for p in split(v))

    cum_col = sums_down(low, a_col)
    cum_row = sum(jnp.dot(p, upp, preferred_element_type=F32) for p in split(a_row))
    lf_col = cum_col[:, 0:1]
    lf_tot = cum_col[T - 1 : T, 0:1]
    lb_tot = cum_col[T - 1 : T, 1:2]
    lb_col = lb_tot - cum_col[:, 1:2] + a_col[:, 1:2]
    lf_row = cum_row[0:1]
    lb_row = lb_tot - cum_row[1:2] + a_row[1:2]
    lane_1 = iota((1, 128), 1)
    lbuf[z] = jnp.where(lane_1 == 0, lf_tot, lb_tot)

    def l_send(i, carry):
        remote(lbuf.at[z], lbuf.at[z], ls_, lr_, {"sp": lax.rem(z + far_first(i), Z)}).start()
        return carry

    lax.fori_loop(0, Z - 1, l_send, 0)

    e_up.wait_recv()
    e_down.wait_recv()

    def conv(v, before, after, taps, rows):
        n = v.shape[0]
        up = jnp.where(rows == 0, before, pltpu.roll(v, 1, 0))
        down = jnp.where(rows == n - 1, after, pltpu.roll(v, n - 1, 0))
        return silu(taps[0] * up + taps[1] * v + taps[2] * down)

    def taps_of(ref):
        rows = [ref[i : i + 1, :].astype(F32) for i in range(3)]
        if rows[0].shape[1] < 128:
            rows = [jnp.concatenate([r, jnp.zeros_like(r)], 1) for r in rows]
        return rows

    tx, tb, tc = taps_of(cx_ref), taps_of(cb_ref), taps_of(cc_ref)
    sub_t = iota((T, 128), 0)
    has_prev = (z > 0).astype(F32)
    has_next = (z < Z - 1).astype(F32)
    e_prev = ebuf[0].astype(F32)[7:8] * has_prev
    e_next = ebuf[1].astype(F32)[0:1] * has_next

    def seg(i):
        return acc[:, i * 128 : i * 128 + 128].astype(BF16).astype(F32)

    def edges(e, i):
        return e[:, i * 128 : i * 128 + 128]

    xz = seg(0)
    xs = conv(xz, edges(e_prev, 0), edges(e_next, 0), tx, sub_t)
    bs = conv(seg(1), edges(e_prev, 1), edges(e_next, 1), tb, sub_t)
    cs = conv(seg(2), edges(e_prev, 2), edges(e_next, 2), tc, sub_t)
    bs_b = bs.astype(BF16)
    cs_b = cs.astype(BF16)


    def state_of(v, writes, wf, wb, lanes):
        doubled = v + pltpu.roll(v, 64, 1)
        return bdot(doubled * jnp.where(lanes < 64, wf, wb), writes, tn)

    st = state_of(
        xs, bs_b,
        jnp.exp(lf_tot - lf_col) * step_col[:, 0:1],
        jnp.exp(lb_tot - lb_col) * step_col[:, 1:2],
        lane_t,
    )
    snd[...] = st.reshape(2, 64, 128).astype(BF16)
    cst[...] = jnp.zeros_like(cst)

    @pl.when((z == 0) | (z == Z - 1))
    def _():
        drain(cbuf, Z - 1, csr)
        cin = cbuf[...].astype(F32).reshape(CT, 256)
        sub_c = iota((CT, 128), 0)
        lane_ct = iota((CT, 128), 1)
        zero_row = jnp.zeros((1, 128), F32)
        xs_c = conv(cin[:, 0:128], zero_row, zero_row, tx, sub_c)
        bs_c = conv(cin[:, 128:256], zero_row, zero_row, tb, sub_c)
        step_c = softplus(cin[:, 0:128] + jnp.where(lane_ct == 64, b0, b1))
        a_c = -step_c * jnp.exp(jnp.where(lane_ct == 64, d0, d1))
        q_c = iota((CT, CT), 0)
        s_c = iota((CT, CT), 1)
        cf_col = sums_down((s_c <= q_c).astype(BF16), a_c)[:, 64:65]
        cb_col = sums_down((s_c >= q_c).astype(BF16), a_c)[:, 65:66]
        states = state_of(
            xs_c, bs_c,
            jnp.exp(cf_col[CT - 1 : CT] - cf_col) * step_c[:, 64:65],
            jnp.exp(cb_col[0:1] - cb_col) * step_c[:, 65:66],
            lane_ct,
        )
        cst[...] = states
        snd[...] = (st + states * jnp.where(sub128 < 64, jnp.exp(lf_tot), jnp.exp(lb_tot))).reshape(2, 64, 128).astype(BF16)

    def s_send(i, carry):
        k = lax.rem(z + far_first(i), Z)
        back = (k < z).astype(jnp.int32)
        remote(snd.at[back], rst.at[z], sts, str_, {"sp": k}).start()
        return carry

    lax.fori_loop(0, Z - 1, s_send, 0)

    pf = jnp.where(s_i <= q_i, jnp.exp(jnp.minimum(lf_col - lf_row, 0.0)), 0.0) * step_row[0:1]
    pb = jnp.where(s_i >= q_i, jnp.exp(jnp.minimum(lb_col - lb_row, 0.0)), 0.0) * step_row[1:2]
    inter = bdot(cs_b, bs_b, nt)
    y_in = bdot(inter * (pf + pb), xs)

    wocopy.wait_recv()

    def join_o(i, carry):
        span = pl.ds(pl.multiple_of(i * 128, 128), 128)
        wo[span, :] = wot[:, span].T
        return carry

    lax.fori_loop(0, D // 128, join_o, 0)

    drain(lbuf, Z - 1, lr_)
    drain(rst, Z - 1, str_)

    sf = cst[0:64] * (z == 0).astype(F32)
    sb = cst[64:128] * (z == Z - 1).astype(F32)
    runs = jnp.zeros((1, 128), F32)
    for i in range(1, Z):
        kf = lax.rem(z + Z - i, Z)
        kb = lax.rem(z + i, Z)
        okf = (i <= z).astype(F32)
        okb = (z + i < Z).astype(F32)
        w = jnp.exp(runs)
        sf = sf + (w[:, 0:1] * okf) * rst[kf].astype(F32)
        sb = sb + (w[:, 1:2] * okb) * rst[kb].astype(F32)
        runs = runs + jnp.where(lane_1 == 0, lbuf[kf] * okf, lbuf[kb] * okb)

    carried = bdot(cs_b, jnp.concatenate([sf, sb], 0), nt) * jnp.where(lane_t < 64, jnp.exp(lf_col), jnp.exp(lb_col))
    ys = y_in + carried + pltpu.roll(carried, 64, 1)
    zin = pltpu.roll(xz, 64, 1)
    g = jnp.where(lane_t < 64, ys * silu(zin), 0.0)
    hg = hg_ref[...].astype(F32)
    hg = jnp.concatenate([hg, jnp.zeros_like(hg)], 1)
    heads = g * lax.rsqrt(jnp.sum(g * g, axis=1, keepdims=True) / 64 + EPS) * hg
    heads = jnp.where(first_core, heads, pltpu.roll(heads, 64, 1))

    osend[...] = jnp.where(first_core, heads[TH:T], heads[0:TH]).astype(BF16)
    op = remote(osend, orecv, ops, opr, partner)
    op.start()
    keep = jnp.where(first_core, heads[0:TH], heads[TH:T])
    op.wait_recv()
    joined = (keep + orecv[...].astype(F32)).astype(BF16)
    obuf[chip] = joined.reshape(TH // 8, 8, 128)
    acco[...] = jnp.zeros_like(acco)

    nb_out, _ = groups(obuf)
    TB = nb_out * 8

    def row_dot(row):
        rows = jnp.concatenate([obuf[row * X + j, 0:nb_out].reshape(TB, 128) for j in range(X)], 1)
        span = pl.ds(pl.multiple_of(row * (X * 128), 128), X * 128)
        acco[0:TB] += jnp.dot(rows, wo[span, :], preferred_element_type=F32)

    gather(obuf, ogs, ogy, ogx, oga, ogb, lambda: None, row_dot)
    rest = jnp.concatenate([obuf[k, nb_out:].reshape(TH - TB, 128) for k in range(NC)], 1)
    acco[TB:] = jnp.dot(rest, wo[...], preferred_element_type=F32)
    upd = acco[...] * mpair[4:5]
    ubuf[...] = upd.reshape(TH // 8, 8, 128).astype(BF16)

    in_half = chip // HC == c

    def u_row(i, carry):
        r = lax.rem(lax.rem(y, Y // 2) + i, Y // 2)
        yy = c * (Y // 2) + r
        for d in range(X):
            xx = lax.rem(x + d, X)
            for e in range(2):
                copy = remote(
                    ubuf.at[r * X + xx], rbuf.at[chip], us, ur,
                    {"tp_0": yy, "tp_1": xx, "tp_2": c if e == 0 else 1 - c},
                )
                if d == 0 and e == 0:

                    @pl.when(yy != y)
                    def _():
                        copy.start()
                else:
                    copy.start()
        return carry

    lax.fori_loop(0, Y // 2, u_row, 0)

    @pl.when(in_half)
    def _():
        rbuf[chip] = ubuf[lax.rem(chip, HC)]

    @pl.when(in_half)
    def _():
        drain(rbuf, NC - 1, ur)

    @pl.when(jnp.logical_not(in_half))
    def _():
        drain(rbuf, NC, ur)

    def finish(k, carry):
        cols = pl.ds(pl.multiple_of(k * 128, 128), 128)
        v = rbuf[k].astype(F32)
        v = jnp.where(first_core, v[0:4], v[4:8])
        out_ref[:, cols] = (lat_ref[:, cols].astype(F32) + v).astype(BF16)
        return carry

    lax.fori_loop(0, NC, finish, 0)

    lp.wait_send()
    wocopy.wait_send()
    e_up.wait_send()
    e_down.wait_send()
    op.wait_send()
    drain(mbuf, Z - 1, m1s)
    drain(sbuf, NC - 1, m2s)
    gather_drain(mine, lgs)
    drain(mine, NC, ld_s)

    @pl.when(z > 0)
    def _():
        c_first.wait_send()

    @pl.when(z < Z - 1)
    def _():
        c_last.wait_send()

    drain(lbuf, Z - 1, ls_)
    drain(rst, Z - 1, sts)
    gather_drain(obuf, ogs)

    @pl.when(in_half)
    def _():
        drain(rbuf, NC - 1, us)

    @pl.when(jnp.logical_not(in_half))
    def _():
        drain(rbuf, NC, us)


def per_device(sizes, latent, context, cond, cond_ctx, wsh, wsc, wga, gain, pz, px, pb, pc, pdt, cx, cb, cc, dtb, dlog, hg, po):
    Z, Y, X = sizes
    NC = Y * X
    D = latent.shape[1]
    T = 8 * NC
    CZ = context.shape[0]
    if pdt.shape[1] < 128:
        pdt = jnp.pad(pdt, ((0, 0), (0, 128 - pdt.shape[1])))
    V = pltpu.VMEM

    def lines(v):
        return (v.size // 128, 128)

    S = pltpu.SemaphoreType.DMA
    vm = pl.BlockSpec(memory_space=pltpu.VMEM)
    hb = pl.BlockSpec(memory_space=pl.ANY)
    one = S
    return pl.pallas_call(
        functools.partial(kernel, sizes),
        out_shape=jax.ShapeDtypeStruct(latent.shape, BF16),
        in_specs=[hb] * 20,
        out_specs=vm,
        scratch_shapes=[
            V((4, D), BF16), V((CZ, D), BF16), V(lines(cond), BF16), V(lines(cond), BF16),
            V((64, D // Z), BF16), V((64, D // Z), BF16), V((64, D // Z), BF16), V(lines(gain), BF16),
            V((3, 64), BF16), V((3, 128), BF16), V((3, 128), BF16), V((1, 2), F32), V((1, 2), F32), V((1, 64), BF16),
            V((D, 512), BF16), V((128, D), BF16), V((128, D), BF16), V((D, 128), BF16),
            V((2, NC, D // 256, 8, 128), BF16), V((4, D // 2), BF16), V((4, D // 2), BF16), V((5, 128), F32), V((5, 128), F32),
            V((Z, 5, 128), F32), V((NC, 4, 128), F32), V((T, 512), F32), V((T // 2, 128), F32),
            V((Z, CZ, 256), BF16), V((2, 8, 384), BF16), V((2, 8, 384), BF16), V((Z, 1, 128), F32),
            V((2, 64, 128), BF16), V((Z, 64, 128), BF16), V((T // 2, 128), BF16), V((T // 2, 128), BF16),
            V((NC, T // 16, 8, 128), BF16), V((T // 16, 8, 128), BF16), V((NC, 8, 128), BF16), V((128, 128), F32), V((2, NC, 8, 128), F32),
            S((20,)), one, one, one, one, one, one, one, one, one, one, one, S((Y,)), S((Y,)), S((X,)), one, one, S((Y,)), one,
            S((2,)), one, S((2,)), S((2,)), one, one, one, one, one, one, one, S((Y,)), S((Y,)), S((X,)), one, one, one,
        ],
        compiler_params=pltpu.CompilerParams(collective_id=0, has_side_effects=True),
        name="mixer",
    )(
        latent, context, cond.reshape(lines(cond)), cond_ctx.reshape(lines(cond)), wsh.T, wsc.T, wga.T, gain.reshape(lines(gain)),
        pz.T, px.T, pb, pc, pdt, cx, cb, cc, dtb.reshape(1, 2), dlog.reshape(1, 2), hg.reshape(1, -1), po.T,
    )


def build(mesh, sizes):
    Z, Y, X = sizes
    torus = Mesh(mesh.devices.reshape(Z, Y, X, 2), SP_TP)
    in_specs = (
        P(SP_TP, None), P("sp", None), P("sp"), P("sp"), P("sp", TP), P("sp", TP), P("sp", TP), P(),
        P(None, TP), P(None, TP), P(None, TP), P(None, TP), P(), P(None, TP), P(None, TP), P(None, TP),
        P(TP), P(TP), P(TP), P(None, TP),
    )
    return jax.shard_map(
        functools.partial(per_device, sizes), mesh=torus, in_specs=in_specs, out_specs=P(SP_TP, None), check_vma=False
    )


def solution(mesh):
    return build(mesh, (mesh.shape["sp"], 8, 4))
```
